256 devices in a mesh: ep: 16 (over y, x), tp: 16 (over z, core).
Axes of the slice: x: 4, y: 4, z: 8, core: 2. Of those that a mesh axis runs over, the one named last changes fastest.
Arguments:
- tokens: bfloat16 [1024, 4096], P(('ep', 'tp')), may hold values from -6 to 6
- rec_state: float32 [1024, 2048], P('ep', 'tp'), may hold values from -40 to 40
- conv_state: bfloat16 [1024, 3, 2048], P('ep', None, 'tp'), may hold values from -6 to 6
- route_ids: int32 [1024, 4], P('ep'), may hold values from 0 to 15, all different within a row; in each aligned block of 4 rows (0 to 3, 4 to 7, ...) at most 2 rows name the same one
- route_weights: float32 [1024, 4], P(('ep', 'tp')), may hold values from 0.1 to 1
- first_gain: bfloat16 [4096], replicated, may hold values from 0.099609375 to 1.8984375
- proj_input: bfloat16 [4096, 2048], P(None, 'tp'), may hold values from -0.09375 to 0.09375
- proj_gate: bfloat16 [4096, 2048], P(None, 'tp'), may hold values from -0.09375 to 0.09375
- conv_taps: bfloat16 [4, 2048], replicated, may hold values from -1.5 to 1.5
- decay_logit: float32 [2048], replicated, may hold values from 1 to 6
- block_decay: bfloat16 [16, 128, 128], replicated, may hold values from -0.5 to 0.5
- block_input: bfloat16 [16, 128, 128], replicated, may hold values from -0.5 to 0.5
- rec_gain: bfloat16 [2048], replicated, may hold values from 0.099609375 to 1.8984375
- proj_out: bfloat16 [2048, 4096], P('tp'), may hold values from -0.125 to 0.125
- second_gain: bfloat16 [4096], replicated, may hold values from 0.099609375 to 1.8984375
- expert_gate: bfloat16 [16, 4096, 4096], P('ep', None, 'tp'), may hold values from -0.21875 to 0.21875
- expert_up: bfloat16 [16, 4096, 4096], P('ep', None, 'tp'), may hold values from -0.21875 to 0.21875
- expert_down: bfloat16 [16, 4096, 4096], P('ep', 'tp'), may hold values from -0.0234375 to 0.0234375
Outputs:
- result: bfloat16 [1024, 4096], P(('ep', 'tp'))
- new_state: float32 [1024, 2048], P('ep', 'tp')
- new_conv: bfloat16 [1024, 3, 2048], P('ep', None, 'tp')
The draws below stay inside these ranges and needn't reach their ends.
Inputs may be any that keep to these rules, and one draw needn't show every extreme that they name: `route_ids`: each row names 4 different experts; in the rows of one device (aligned blocks of 4 rows) no expert is named by more than 2 rows, and one is named by exactly 2.
All inputs are finite; a program needn't handle non-finite values.
Results may differ from the reference program's by a relative error of at most 0.025.
Values may be sent and summed in bfloat16 or wider, within the bound.
A program may use at most 64 MiB of HBM per device.

```python
import math
import jax
import jax.numpy as jnp
import numpy as np
from jax import lax

D = 4096
D_REC = 2048
REC_BLOCKS = 16
BLOCK_W = 128
TAPS = 4
FF = 4096
EXPERTS = 16
TOP_K = 4
TOK = 4
CAP = 2
BATCH = 1024
N_EP = 16
N_TP = 16


def draw_rec_state(key, part):
    key_base, key_rows = jax.random.split(jax.random.fold_in(key, 11), 2)
    column = jnp.arange(D_REC, dtype=jnp.float32) / D_REC
    column_scale = 0.4 * jnp.exp(column * math.log(8.0))
    row_scale = jnp.exp(jax.random.uniform(key_rows, (BATCH, 1), jnp.float32, math.log(0.3), math.log(3.0)))
    base = jnp.clip(jax.random.normal(key_base, (BATCH, D_REC), jnp.float32), -4.0, 4.0)
    return base * row_scale * column_scale


def steps_of(stream_key, shape, cuts, least, top_value):
    level, own = 1.0, jax.random.fold_in(stream_key, 6)
    for dim, shards_of in cuts:
        draws = jnp.exp(jax.random.uniform(jax.random.fold_in(own, dim), (shards_of,), jnp.float32, least / len(cuts), top_value / len(cuts)))
        level = level * jnp.repeat(draws, shape[dim] // shards_of).reshape([-1 if axis == dim else 1 for axis in range(len(shape))])
    return level


def routed_block(own_key, own, number, rows, number_of, top, most, lean):
    order = jax.random.permutation(own_key, number_of)
    packed, common = shares(number_of, rows * top, most, lean, True), shares(number_of, rows * top, most, lean, False)
    places = jnp.arange(number_of)

    def named(lengths, turn):
        used = int((lengths > 0).sum())
        fixed = max(1, used // 4)
        passed = fixed + (places - fixed + turn * (used - fixed)) % max(1, number_of - fixed)
        return jnp.zeros((number_of,), jnp.int32).at[order[jnp.where(places < fixed, places, passed)]].set(jnp.asarray(lengths, jnp.int32))

    lengths = jnp.where(number % 4 == 0, named(packed, number // 4), named(common, number - number // 4 - 1))
    mixed = jax.random.permutation(jax.random.fold_in(own, 3), number_of)
    donor, receiver = mixed[0:number_of // 2 * 2:2], mixed[1:number_of // 2 * 2:2]
    room = jnp.minimum(lengths[donor] - 1, most - lengths[receiver]) // 2
    room = jnp.where((donor == order[0]) | (receiver == order[0]) | (lengths[receiver] == 0), 0, jnp.maximum(room, 0))
    passed = jax.random.randint(jax.random.fold_in(own, 4), (number_of // 2,), 0, 1 << 20) % (room + 1)
    lengths = lengths.at[donor].add(-passed).at[receiver].add(passed)
    labels = jnp.searchsorted(jnp.cumsum(lengths), jnp.arange(rows * top), side="right").astype(jnp.int32)
    table = labels.reshape(top, rows).T
    table = table[jax.random.permutation(jax.random.fold_in(own, 1), rows)]
    turn = jax.random.randint(jax.random.fold_in(own, 2), (rows, 1), 0, top)
    return jnp.take_along_axis(table, (jnp.arange(top)[None, :] + turn) % top, axis=1)


def shares(count, total, limit, slope, full):
    loads = [(1 << 20) // math.isqrt(grade ** slope) + 1 for grade in range(1, count + 1)]
    largest = limit if full else min(limit, max(-(-total // count), total * loads[0] // sum(loads)))
    least = 1 if total - largest >= count - 1 else 0
    counts, rest = [largest] + [least] * (count - 1), total - largest - least * (count - 1)
    while rest > 0:
        movable = [i for i in range(1, count) if counts[i] < largest] or [i for i in range(1, count) if counts[i] < limit]
        pool, remaining = sum([loads[i] for i in movable]), rest
        for i in movable:
            extra = min(limit - counts[i], max(1, remaining * loads[i] // pool), rest)
            counts[i] = counts[i] + extra
            rest = rest - extra
    return np.array(counts)


def centred(own_key, extent, width, most, cuts=(), held_as=jnp.bfloat16):
    loudness = steps_of(own_key, extent, cuts, -0.22, 0.18) if cuts else 1.0
    entries = jax.random.normal(own_key, extent, jnp.float32) * width * loudness
    return jnp.minimum(jnp.maximum(entries, -most), most).astype(held_as)


def setup_inputs(seed: int = 0) -> dict:
    seeds = jax.random.split(jax.random.key(seed), 19)
    tokens = centred(seeds[0], (BATCH, D), 1.0, 6.0, ((0, 256),))
    rec_state = draw_rec_state(jax.random.fold_in(seeds[18], 71), 0)
    conv_state = centred(seeds[2], (BATCH, TAPS - 1, D_REC), 1.0, 6.0, ((0, 16), (2, 16)))
    route_ids_keys = jax.random.split(jax.random.fold_in(seeds[3], 1), BATCH // TOK)
    route_ids_turns = jax.random.permutation(jax.random.fold_in(seeds[3], 3), BATCH // TOK)
    route_ids = jax.vmap(lambda own, number: routed_block(jax.random.fold_in(seeds[3], 2), own, number, TOK, EXPERTS, TOP_K, CAP, 1))(route_ids_keys, route_ids_turns).reshape((BATCH, TOP_K))
    route_weights = jnp.clip(jnp.exp(math.log(1.0) - 2.3025851 * jax.random.uniform(seeds[4], (BATCH, TOP_K), jnp.float32) ** steps_of(seeds[4], (BATCH, TOP_K), ((0, 256),), -0.2, 0.2)), 0.1, 1.0)
    first_gain = jnp.clip(1.0 + 0.18 * jax.random.normal(seeds[5], (D,), jnp.float32), 0.099609375, 1.8984375).astype(jnp.bfloat16)
    proj_input = centred(seeds[6], (D, D_REC), D ** -0.5, 0.09375, ((1, 16),))
    proj_gate = centred(seeds[7], (D, D_REC), D ** -0.5, 0.09375, ((1, 16),))
    conv_taps = centred(seeds[8], (TAPS, D_REC), 0.25, 1.5)
    decay_logit = jnp.clip(jax.random.uniform(seeds[9], (D_REC,), jnp.float32, 1.0, 6.0), 1.0, 6.0)
    block_decay = centred(seeds[10], (REC_BLOCKS, BLOCK_W, BLOCK_W), BLOCK_W ** -0.5, 0.5)
    block_input = centred(seeds[11], (REC_BLOCKS, BLOCK_W, BLOCK_W), BLOCK_W ** -0.5, 0.5)
    rec_gain = jnp.clip(1.0 + 0.18 * jax.random.normal(seeds[12], (D_REC,), jnp.float32), 0.099609375, 1.8984375).astype(jnp.bfloat16)
    proj_out = centred(seeds[13], (D_REC, D), D_REC ** -0.5, 0.125, ((0, 16),))
    second_gain = jnp.clip(1.0 + 0.18 * jax.random.normal(seeds[14], (D,), jnp.float32), 0.099609375, 1.8984375).astype(jnp.bfloat16)
    expert_gate = centred(seeds[15], (EXPERTS, D, FF), (D // 6) ** -0.5, 0.21875, ((0, 16), (2, 16)))
    expert_up = centred(seeds[16], (EXPERTS, D, FF), (D // 6) ** -0.5, 0.21875, ((0, 16), (2, 16)))
    expert_down = centred(seeds[17], (EXPERTS, FF, D), (FF * 16) ** -0.5, 0.0234375, ((0, 16), (1, 16)))
    return dict(tokens=tokens, rec_state=rec_state, conv_state=conv_state, route_ids=route_ids, route_weights=route_weights, first_gain=first_gain, proj_input=proj_input, proj_gate=proj_gate, conv_taps=conv_taps, decay_logit=decay_logit, block_decay=block_decay, block_input=block_input, rec_gain=rec_gain, proj_out=proj_out, second_gain=second_gain, expert_gate=expert_gate, expert_up=expert_up, expert_down=expert_down)


EPS = 1e-06
CLAMP = 7.0
ALPHA = 1.702
RATE = 8.0

def norm_rows(values, gain):
    scale = lax.rsqrt(lax.optimization_barrier(jnp.mean(values * values, axis=-1, keepdims=True)) + EPS)
    return values * scale * gain.astype(jnp.float32)

def slot_positions(ids, blocks):
    rows, picks = ids.shape
    onehot = (ids[:, :, None] == jnp.arange(EXPERTS, dtype=jnp.int32)).astype(jnp.int32)
    onehot = onehot.reshape(blocks, rows // blocks * picks, EXPERTS)
    before = jnp.cumsum(onehot, axis=1) - onehot
    return lax.optimization_barrier(jnp.sum(before * onehot, axis=-1)).reshape(rows, picks).astype(jnp.int32)

def reference(tokens, rec_state, conv_state, route_ids, route_weights, first_gain, proj_input, proj_gate, conv_taps, decay_logit, block_decay, block_input, rec_gain, proj_out, second_gain, expert_gate, expert_up, expert_down):
    token_values = tokens.astype(jnp.float32)
    normed = norm_rows(token_values, first_gain).astype(jnp.bfloat16)
    branch_in = jnp.dot(normed, proj_input, preferred_element_type=jnp.float32).astype(jnp.bfloat16)
    branch_gate = jnp.dot(normed, proj_gate, preferred_element_type=jnp.float32).astype(jnp.bfloat16)
    tap_weights = conv_taps.astype(jnp.float32)
    conv_values = conv_state.astype(jnp.float32)
    conv_out = tap_weights[TAPS - 1] * branch_in.astype(jnp.float32)
    for tap in range(TAPS - 1):
        conv_out = conv_out + tap_weights[tap] * conv_values[:, tap]
    new_conv = jnp.concatenate([conv_state[:, 1:], branch_in[:, None, :]], axis=1)
    conv_low = lax.optimization_barrier(conv_out.astype(jnp.bfloat16)).astype(jnp.float32)
    blocked = conv_low.reshape(BATCH, REC_BLOCKS, BLOCK_W)
    decay_gate = jax.nn.sigmoid(jnp.einsum('rnk,nkj->rnj', blocked, block_decay.astype(jnp.float32)).reshape(BATCH, D_REC))
    input_gate = jax.nn.sigmoid(jnp.einsum('rnk,nkj->rnj', blocked, block_input.astype(jnp.float32)).reshape(BATCH, D_REC))
    log_keep = -RATE * decay_gate * jax.nn.softplus(-decay_logit)
    keep_factor = jnp.exp(log_keep)
    new_state = keep_factor * rec_state + jnp.sqrt(-jnp.expm1(2.0 * log_keep)) * input_gate * conv_out
    hidden = new_state * jax.nn.gelu(branch_gate.astype(jnp.float32))
    squares = lax.optimization_barrier(jnp.sum(hidden * hidden, axis=-1, keepdims=True))
    gained = (hidden * rec_gain.astype(jnp.float32)).astype(jnp.bfloat16)
    partial_value = jnp.dot(gained, proj_out, preferred_element_type=jnp.float32)
    residual = token_values + partial_value * lax.rsqrt(squares / D_REC + EPS)
    second = norm_rows(residual, second_gain).astype(jnp.bfloat16)
    devices = N_EP * N_TP
    tok_rows = BATCH // devices
    positions = slot_positions(route_ids, devices)
    row_owner = (jnp.arange(BATCH, dtype=jnp.int32) // tok_rows)[:, None]
    slots = row_owner * CAP + positions
    slot_count = devices * CAP
    row_index = jnp.broadcast_to(jnp.arange(BATCH, dtype=jnp.int32)[:, None], route_ids.shape)
    table = jnp.zeros((EXPERTS, slot_count), jnp.int32).at[route_ids, slots].set(row_index)

    def run_expert(expert):
        rows_in = second[table[expert]]
        gate = jnp.dot(rows_in, expert_gate[expert], preferred_element_type=jnp.float32)
        upper = jnp.dot(rows_in, expert_up[expert], preferred_element_type=jnp.float32)
        clipped = jnp.minimum(gate, CLAMP)
        act = ((jnp.clip(upper, -CLAMP, CLAMP) + 1.0) * (clipped * jax.nn.sigmoid(ALPHA * clipped))).astype(jnp.bfloat16)
        pieces = jnp.einsum('rtf,tfd->rtd', act.reshape(slot_count, N_TP, FF // N_TP).astype(jnp.float32), expert_down[expert].reshape(N_TP, FF // N_TP, D).astype(jnp.float32))
        rounded = lax.optimization_barrier(pieces.astype(jnp.bfloat16)).astype(jnp.float32)
        return lax.optimization_barrier(jnp.sum(rounded, axis=1)).astype(jnp.bfloat16)
    outputs = lax.map(run_expert, jnp.arange(EXPERTS, dtype=jnp.int32))
    picked = outputs[route_ids, slots].astype(jnp.float32)
    expert_mix = lax.optimization_barrier(jnp.sum(route_weights[:, :, None] * picked, axis=1))
    result = (residual + expert_mix).astype(jnp.bfloat16)
    return (result, new_state, new_conv)
```

```python
import jax
import jax.numpy as jnp
from jax import lax
from jax.experimental import pallas as pl
from jax.experimental.pallas import tpu as pltpu
from jax.sharding import PartitionSpec as P

MESH = pl.DeviceIdType.MESH
BF16, F32, I32 = jnp.bfloat16, jnp.float32, jnp.int32

EPS = 1e-06
CLAMP = 7.0
ALPHA = 1.702
RATE = 8.0

D = 4096
NC = 4
CW = D // NC
TOK = 4
NE = 16
NT = 16
NZ = 8
D_REC = 2048
W = 128
FW = 256
SLOTS = 2
ROWS = NE * SLOTS
HALF = ROWS // 2
TAIL = 128


def iota(shape, dim):
    return lax.broadcasted_iota(I32, shape, dim)


def onehot(cond):
    return jnp.where(cond, 1.0, 0.0).astype(F32)


def dot(a, b):
    return jnp.dot(a, b, preferred_element_type=F32)


def per_token(values):
    part = jnp.broadcast_to(jnp.sum(values, axis=1, keepdims=True), (NC * TOK, 128))
    total = part
    for c in range(1, NC):
        total = total + pltpu.roll(part, c * TOK, 0)
    return total[:, 0:1]


def spread(row_ref):
    c_of = iota((NC * TOK, CW), 0) // TOK
    out = jnp.zeros((NC * TOK, CW), F32)
    for c in range(NC):
        piece = row_ref[:, c * CW : (c + 1) * CW].astype(F32)
        out = jnp.where(c_of == c, jnp.broadcast_to(piece, (NC * TOK, CW)), out)
    return out


def minus_expm1(x):
    small = jnp.full_like(x, 1.0)
    for k in range(8, 1, -1):
        small = 1.0 + small * x * (1.0 / k)
    return jnp.where(x > -0.3, -x * small, 1.0 - jnp.exp(x))


def kernel(
    tokens_ref, rec_ref, conv_ref, ids_ref, weights_ref, gain1_ref, taps_ref, logit_ref, rgain_ref, gain2_ref,
    pin_hbm, pgate_hbm, bdec_hbm, binp_hbm, pout_hbm, eg_hbm, eu_hbm, ed_hbm,
    result_ref, state_ref, newconv_ref,
    wcat, w4, bdec, binp, wgu, wdown,
    tok_s, g1, pb, rp, sb, rb, ob, ib, xg, part, rpart, sums, rright, rleft, ob2, ib2, rw_s,
    lsem, s1, r1, s2p, r2p, s2, r2, s3, r3, s4, r4, s4d, r4d, s5p, r5p, s5, r5r, r5l, s6, r6,
):
    ep = lax.axis_index("ep")
    tp = lax.axis_index("tp")
    z = tp // 2
    core = tp % 2
    other = 1 - core
    mate = (ep, z * 2 + other)

    def along(d):
        return (z + d + NZ) % NZ

    def at_z(zz):
        return (ep, zz * 2 + core)

    barrier = pltpu.get_barrier_semaphore()
    pl.semaphore_signal(barrier, inc=1, device_id=mate, device_id_type=MESH)
    for d in range(1, NZ):
        pl.semaphore_signal(barrier, inc=1, device_id=at_z(along(d)), device_id_type=MESH)
    for d in range(1, NE):
        pl.semaphore_signal(barrier, inc=1, device_id=((ep + d) % NE, tp), device_id_type=MESH)

    loads = [
        pltpu.make_async_copy(pin_hbm, wcat.at[:, pl.ds(0, W)], lsem.at[0]),
        pltpu.make_async_copy(pgate_hbm, wcat.at[:, pl.ds(W, W)], lsem.at[1]),
        pltpu.make_async_copy(bdec_hbm.at[tp], bdec, lsem.at[2]),
        pltpu.make_async_copy(binp_hbm.at[tp], binp, lsem.at[3]),
    ]
    for c in range(NC):
        loads.append(
            pltpu.make_async_copy(
                pout_hbm.at[:, pl.ds(c * CW, CW)], w4.at[pl.ds(c * W, W), :], lsem.at[4 + c]
            )
        )
    loads.append(pltpu.make_async_copy(eg_hbm.at[0], wgu.at[:, pl.ds(0, FW)], lsem.at[8]))
    loads.append(pltpu.make_async_copy(eu_hbm.at[0], wgu.at[:, pl.ds(FW, FW)], lsem.at[9]))
    loads.append(pltpu.make_async_copy(ed_hbm.at[0], wdown, lsem.at[10]))
    for load in loads:
        load.start()

    own = tokens_ref[...].astype(F32)
    for c in range(NC):
        tok_s[c * TOK : (c + 1) * TOK, :] = own[:, c * CW : (c + 1) * CW]
    values = tok_s[...]
    scale = lax.rsqrt(per_token(values * values) * (1.0 / D) + EPS)
    g1[tp] = (values * scale * spread(gain1_ref)).astype(BF16)

    pl.semaphore_wait(barrier, NZ + NE - 1)

    def copy1(dev, slot):
        return pltpu.make_async_remote_copy(
            src_ref=g1.at[slot], dst_ref=g1.at[slot], send_sem=s1, recv_sem=r1.at[slot], device_id=dev, device_id_type=MESH
        )

    for d in (4, 3, 5, 2, 6, 1, 7):
        copy1(at_z(along(d)), tp).start()
    copy1(mate, tp).start()

    q4, r4e = (NC * TOK, W), 8
    row_n, row_c = iota(q4, 0) % TOK, iota(q4, 0) // TOK
    lane_e, lane_c, lane_s = iota(q4, 1) // r4e, (iota(q4, 1) // SLOTS) % NC, iota(q4, 1) % SLOTS
    pick_own = onehot(iota((NC * TOK, NE * TOK), 1) == tp * TOK + iota((NC * TOK, NE * TOK), 0) % TOK)
    own_ids = dot(pick_own.astype(BF16), ids_ref[...].astype(F32).astype(BF16))
    for c in range(NC):
        rw_s[c * TOK : (c + 1) * TOK, :] = weights_ref[...]
    hit = jnp.zeros(q4, F32)
    weighed = jnp.zeros(q4, F32)
    lane_ef = lane_e.astype(F32)
    for k in range(4):
        same = onehot(own_ids[:, k : k + 1] == lane_ef)
        hit = hit + same
        weighed = weighed + same * rw_s[:, k : k + 1]
    sq = (NC * TOK, NC * TOK)
    earlier = onehot(
        (iota(sq, 0) // TOK == iota(sq, 1) // TOK) & (iota(sq, 1) % TOK < iota(sq, 0) % TOK)
    )
    before = dot(earlier.astype(BF16), hit.astype(BF16))
    chosen = hit * onehot((before == lane_s.astype(F32)) & (row_c == lane_c))
    combine = chosen * weighed

    for d in (1, 7, 2, 6, 3, 5, 4):
        slot = along(d) * 2 + core
        copy1(mate, slot).wait_recv()
        copy1(mate, slot).start()
    for d in range(NZ):
        copy1(mate, along(d) * 2 + other).wait_recv()

    big = NT * NC * TOK
    pr, pc = iota((big, big), 0), iota((big, big), 1)
    perm = onehot(pc == ((pr // TOK) % NT) * 16 + (pr // 64) * TOK + pr % TOK).astype(BF16)
    stacked = dot(perm, g1[...].reshape(big, CW)).astype(BF16)
    for load in loads[0:4]:
        load.wait()
    both = jnp.zeros((NT * TOK, 2 * W), F32)
    for c in range(NC):
        both = both + dot(stacked[c * 64 : (c + 1) * 64, :], wcat[c * CW : (c + 1) * CW, :])
    joined = both.astype(BF16)
    branch_in, branch_gate = joined[:, :W].astype(F32), joined[:, W:].astype(F32)

    taps = taps_ref[:, pl.ds(pl.multiple_of(tp * W, W), W)].astype(F32)
    conv = taps[3:4, :] * branch_in
    for tap in range(3):
        conv = conv + taps[tap : tap + 1, :] * conv_ref[:, tap * W : (tap + 1) * W].astype(F32)
    newconv_ref[:, 0 : 2 * W] = conv_ref[:, W : 3 * W]
    newconv_ref[:, 2 * W : 3 * W] = joined[:, :W]

    low = conv.astype(BF16)
    decay_gate = jax.nn.sigmoid(dot(low, bdec[...]))
    input_gate = jax.nn.sigmoid(dot(low, binp[...]))
    mine = iota((NT, W), 0) == tp
    logit = jnp.sum(jnp.where(mine, logit_ref[...], 0.0), axis=0, keepdims=True)
    rgain = jnp.sum(jnp.where(mine, rgain_ref[...].astype(F32), 0.0), axis=0, keepdims=True)
    soft = jnp.maximum(-logit, 0.0) + jnp.log1p(jnp.exp(-jnp.abs(logit)))
    log_keep = -RATE * decay_gate * soft
    new_state = jnp.exp(log_keep) * rec_ref[...] + jnp.sqrt(minus_expm1(2.0 * log_keep)) * input_gate * conv
    state_ref[...] = new_state
    hidden = new_state * jax.nn.gelu(branch_gate)
    squares = jnp.broadcast_to(jnp.sum(hidden * hidden, axis=1, keepdims=True), (NT * TOK, W))

    er, et = iota((big, NT * TOK), 0), iota((big, NT * TOK), 1)
    expand = onehot(et == (((er // 16) % NZ) * 2 + er // 128) * TOK + er % TOK).astype(BF16)
    wide = dot(expand, jnp.concatenate([(hidden * rgain).astype(BF16), squares.astype(BF16)], axis=1))
    gained, sq_wide = wide[:, :W], wide[:, W:]
    c_of = (iota((big, W), 0) // TOK) % NC
    for load in loads[4:8]:
        load.wait()
    lhs = jnp.concatenate([jnp.where(c_of == c, gained, 0.0) for c in range(NC)], axis=1).astype(BF16)
    pb[:, :, :, 0:CW] = dot(lhs, w4[...]).astype(BF16).reshape(2, NZ, 16, CW)
    pb[:, :, :, CW : CW + TAIL] = sq_wide.astype(BF16).reshape(2, NZ, 16, TAIL)

    pair2 = pltpu.make_async_remote_copy(
        src_ref=pb.at[other], dst_ref=rp, send_sem=s2p, recv_sem=r2p, device_id=mate, device_id_type=MESH
    )
    pair2.start()
    pair2.wait_recv()

    def copy2(dev, slot):
        return pltpu.make_async_remote_copy(
            src_ref=sb.at[slot], dst_ref=rb.at[z], send_sem=s2, recv_sem=r2, device_id=dev, device_id_type=MESH
        )

    for d in (4, 3, 5, 2, 6, 1, 7):
        zz = along(d)
        sb[zz] = (pb[core, zz].astype(F32) + rp[zz].astype(F32)).astype(BF16)
        copy2(at_z(zz), zz).start()
    rb[z] = (pb[core, z].astype(F32) + rp[z].astype(F32)).astype(BF16)
    pltpu.make_async_copy(sb.at[pl.ds(0, NZ - 1)], rb.at[pl.ds(0, NZ - 1)], r2).wait()
    summed = jnp.zeros((16, CW + TAIL), F32)
    for zz in range(NZ):
        summed = summed + rb[zz].astype(F32)
    residual = tok_s[...] + summed[:, :CW] * lax.rsqrt(summed[:, CW : CW + 1] * (1.0 / D_REC) + EPS)
    scale = lax.rsqrt(per_token(residual * residual) * (1.0 / D) + EPS)
    second = (residual * scale * spread(gain2_ref)).astype(BF16)
    tok_s[...] = residual

    sent = lax.dot_general(chosen.astype(BF16), second, (((0,), (0,)), ((), ())), preferred_element_type=F32)
    ob[...] = sent.reshape(NE, 8, CW).astype(BF16)
    ib[ep] = ob[ep]

    def copy3(e, src, dst, ss, rs):
        return pltpu.make_async_remote_copy(
            src_ref=src.at[e], dst_ref=dst.at[ep], send_sem=ss, recv_sem=rs, device_id=(e, tp), device_id_type=MESH
        )

    far = (10, 6, 14, 9, 11, 5, 7, 13, 15, 2, 8, 1, 3, 4, 12)
    for d in far:
        copy3((ep + d) % NE, ob, ib, s3, r3).start()
    for load in loads[8:]:
        load.wait()
    pltpu.make_async_copy(ob.at[pl.ds(0, NE - 1)], ib.at[pl.ds(0, NE - 1)], r3).wait()
    own_rows = NE * 8
    sr, sc = iota((own_rows, own_rows), 0), iota((own_rows, own_rows), 1)
    turn = onehot(sc == ((sr // SLOTS) % NE) * 8 + (sr // ROWS) * SLOTS + sr % SLOTS).astype(BF16)
    turned = dot(turn, ib[...].astype(F32).reshape(own_rows, CW).astype(BF16)).astype(BF16)
    for c in range(NC):
        xg[z, core, :, c * CW : (c + 1) * CW] = turned[c * ROWS : (c + 1) * ROWS, :]

    def copy4(zz, h, dev):
        block = xg.at[zz, core, pl.ds(h * HALF, HALF), :]
        return pltpu.make_async_remote_copy(
            src_ref=block, dst_ref=block, send_sem=s4, recv_sem=r4.at[zz * 2 + h], device_id=dev, device_id_type=MESH
        )

    def cross4(zz, h, side):
        block = xg.at[zz, side, pl.ds(h * HALF, HALF), :]
        return pltpu.make_async_remote_copy(
            src_ref=block, dst_ref=block, send_sem=s4d, recv_sem=r4d.at[zz * 2 + h], device_id=mate, device_id_type=MESH
        )

    right, left = at_z(along(1)), at_z(along(-1))
    for h in range(2):
        copy4(z, h, right).start()
        copy4(z, 1 - h, left).start()
    for h in range(2):
        cross4(z, h, core).start()

    def run_expert(zz):
        for h in range(2):
            cross4(zz, h, other).wait_recv()
        rows = xg[zz].reshape(2 * ROWS, D)
        gu = dot(rows, wgu[...])
        gate, up = jnp.minimum(gu[:, :FW], CLAMP), jnp.clip(gu[:, FW:], -CLAMP, CLAMP)
        act = ((up + 1.0) * (gate * jax.nn.sigmoid(ALPHA * gate))).astype(BF16)
        part[zz] = dot(act, wdown[...]).astype(BF16).reshape(2, ROWS, D)
        pltpu.make_async_remote_copy(
            src_ref=part.at[zz, other], dst_ref=rpart.at[zz], send_sem=s5p, recv_sem=r5p.at[zz], device_id=mate, device_id_type=MESH
        ).start()

    for s in range(1, 5):
        for h in range(2):
            for way, hops, nxt in ((-1, 4 - h, right), (1, 3 + h, left)):
                if s <= hops:
                    zz = along(way * s)
                    copy4(zz, h, nxt).wait_recv()
                    if s < hops:
                        copy4(zz, h, nxt).start()
                    cross4(zz, h, core).start()
        if s == 1:
            run_expert(z)
        else:
            pl.loop(0, 2)(lambda i, s=s: run_expert(along((s - 1) * (1 - 2 * i))))
    run_expert(along(4))

    def pair_sum(zz, h):
        rows = slice(h * HALF, (h + 1) * HALF)
        return part[zz, core, rows, :].astype(F32) + rpart[zz, rows, :].astype(F32)

    def wait_pair(zz):
        pltpu.make_async_remote_copy(
            src_ref=part.at[zz, other], dst_ref=rpart.at[zz], send_sem=s5p, recv_sem=r5p.at[zz], device_id=mate, device_id_type=MESH
        ).wait_recv()

    def copy5(zz, h, hop, to_right):
        return pltpu.make_async_remote_copy(
            src_ref=sums.at[zz, h],
            dst_ref=(rright if to_right else rleft).at[h, hop],
            send_sem=s5,
            recv_sem=(r5r if to_right else r5l).at[h * 4 + hop],
            device_id=right if to_right else left,
            device_id_type=MESH,
        )

    def got5(h, hop, from_left):
        return (rright if from_left else rleft)[h, hop].astype(F32)

    for hop in range(4, 0, -1):
        for zz in {4: (along(4),), 3: (along(3), along(-3)), 2: (along(2), along(-2)), 1: (along(1), along(-1))}[hop]:
            wait_pair(zz)
        for h in range(2):
            for to_right, longest in ((True, 4 - h), (False, 3 + h)):
                if hop > longest:
                    continue
                zz = along(hop if to_right else -hop)
                total = pair_sum(zz, h)
                if hop < longest:
                    copy5(zz, h, hop, to_right).wait_recv()
                    total = total + got5(h, hop, to_right)
                sums[zz, h] = total.astype(BF16)
                copy5(zz, h, hop - 1, to_right).start()
    wait_pair(z)
    for h in range(2):
        total = pair_sum(z, h)
        for to_right in (True, False):
            copy5(z, h, 0, to_right).wait_recv()
            total = total + got5(h, 0, to_right)
        sums[z, h] = total.astype(BF16)

    mine = jnp.concatenate([sums[z].reshape(ROWS, D)[:, c * CW : (c + 1) * CW] for c in range(NC)], axis=0)
    back = onehot(sr == ((sc // SLOTS) % NE) * 8 + (sc // ROWS) * SLOTS + sc % SLOTS).astype(BF16)
    ob2[...] = dot(back, mine).reshape(NE, 8, CW).astype(BF16)
    ib2[ep] = ob2[ep]
    for d in far:
        copy3((ep + d) % NE, ob2, ib2, s6, r6).start()
    high = combine.astype(BF16)
    rest = combine - high.astype(F32)
    middle = rest.astype(BF16)
    lowest = (rest - middle.astype(F32)).astype(BF16)
    pltpu.make_async_copy(ob2.at[pl.ds(0, NE - 1)], ib2.at[pl.ds(0, NE - 1)], r6).wait()
    returned = ib2[...].astype(F32).reshape(NE * 8, CW).astype(BF16)
    mix = dot(lowest, returned) + dot(middle, returned) + dot(high, returned)
    tok_s[...] = tok_s[...] + mix
    for c in range(NC):
        result_ref[:, c * CW : (c + 1) * CW] = tok_s[c * TOK : (c + 1) * TOK, :].astype(BF16)

    def drain(ref, sem):
        pltpu.make_async_copy(ref, ref, sem).wait()

    drain(g1.at[pl.ds(0, NT - 1)], s1)
    pair2.wait_send()
    drain(sb.at[pl.ds(0, NZ - 1)], s2)
    drain(ob.at[pl.ds(0, NE - 1)], s3)
    drain(xg.at[pl.ds(0, NZ - 1), 0], s4)
    drain(xg.at[:, 0], s4d)
    drain(rpart, s5p)
    drain(sums.at[pl.ds(0, NZ - 1)], s5)
    drain(ob2.at[pl.ds(0, NE - 1)], s6)


def per_device(
    tokens, rec_state, conv_state, route_ids, route_weights, first_gain, proj_input, proj_gate, conv_taps,
    decay_logit, block_decay, block_input, rec_gain, proj_out, second_gain, expert_gate, expert_up, expert_down,
):
    seqs = rec_state.shape[0]
    vmem, hbm = pl.BlockSpec(memory_space=pltpu.VMEM), pl.BlockSpec(memory_space=pl.ANY)
    dma, v = pltpu.SemaphoreType.DMA, pltpu.VMEM
    result, new_state, new_conv = pl.pallas_call(
        kernel,
        name="layer",
        out_shape=(
            jax.ShapeDtypeStruct(tokens.shape, BF16),
            jax.ShapeDtypeStruct(rec_state.shape, F32),
            jax.ShapeDtypeStruct((seqs, 3 * W), BF16),
        ),
        in_specs=[vmem] * 10 + [hbm] * 8,
        out_specs=(vmem, vmem, vmem),
        scratch_shapes=[
            v((D, 2 * W), BF16), v((NC * W, CW), BF16), v((W, W), BF16), v((W, W), BF16),
            v((D, 2 * FW), BF16), v((FW, D), BF16),
            v((16, CW), F32), v((NT, 16, CW), BF16),
            v((2, NZ, 16, CW + TAIL), BF16), v((NZ, 16, CW + TAIL), BF16), v((NZ, 16, CW + TAIL), BF16),
            v((NZ, 16, CW + TAIL), BF16),
            v((NE, 8, CW), BF16), v((NE, 8, CW), BF16),
            v((NZ, 2, ROWS, D), BF16), v((NZ, 2, ROWS, D), BF16), v((NZ, ROWS, D), BF16),
            v((NZ, 2, HALF, D), BF16), v((2, 4, HALF, D), BF16), v((2, 4, HALF, D), BF16),
            v((NE, 8, CW), BF16), v((NE, 8, CW), BF16), v((16, 4), F32),
            dma((11,)), dma, dma((NT,)), dma, dma, dma, dma, dma, dma,
            dma, dma((NZ * 2,)), dma, dma((NZ * 2,)), dma, dma((NZ,)), dma, dma((8,)), dma((8,)), dma, dma,
        ],
        compiler_params=pltpu.CompilerParams(
            collective_id=0, has_side_effects=True, vmem_limit_bytes=60 * 1024 * 1024
        ),
    )(
        tokens, rec_state, conv_state.reshape(seqs, 3 * W), route_ids, route_weights, first_gain.reshape(1, D),
        conv_taps, decay_logit.reshape(NT, W), rec_gain.reshape(NT, W), second_gain.reshape(1, D),
        proj_input, proj_gate, block_decay, block_input, proj_out, expert_gate, expert_up, expert_down,
    )
    return result, new_state, new_conv.reshape(seqs, 3, W)


def solution(mesh):
    in_specs = (
        P(("ep", "tp"), None),
        P("ep", "tp"),
        P("ep", None, "tp"),
        P("ep", None),
        P(("ep", "tp"), None),
        P(),
        P(None, "tp"),
        P(None, "tp"),
        P(),
        P(),
        P(),
        P(),
        P(),
        P("tp", None),
        P(),
        P("ep", None, "tp"),
        P("ep", None, "tp"),
        P("ep", "tp", None),
    )
    out_specs = (P(("ep", "tp"), None), P("ep", "tp"), P("ep", None, "tp"))
    return jax.shard_map(
        per_device, mesh=mesh, in_specs=in_specs, out_specs=out_specs, check_vma=False
    )
```

```python
import jax
import jax.numpy as jnp
from jax import lax
from jax.experimental import pallas as pl
from jax.experimental.pallas import tpu as pltpu
from jax.sharding import PartitionSpec as P

MESH = pl.DeviceIdType.MESH
BF16, F32, I32 = jnp.bfloat16, jnp.float32, jnp.int32

EPS = 1e-06
CLAMP = 7.0
ALPHA = 1.702
RATE = 8.0

D = 4096
NC = 4
CW = D // NC
TOK = 4
NE = 16
NT = 16
NZ = 8
D_REC = 2048
W = 128
FW = 256
SLOTS = 2
ROWS = NE * SLOTS
HALF = ROWS // 2
TAIL = 128


def iota(shape, dim):
    return lax.broadcasted_iota(I32, shape, dim)


def onehot(cond):
    return jnp.where(cond, 1.0, 0.0).astype(F32)


def dot(a, b):
    return jnp.dot(a, b, preferred_element_type=F32)


def per_token(values):
    part = jnp.broadcast_to(jnp.sum(values, axis=1, keepdims=True), (NC * TOK, 128))
    total = part
    for c in range(1, NC):
        total = total + pltpu.roll(part, c * TOK, 0)
    return total[:, 0:1]


def spread(ref):
    values, shape = ref[...].astype(F32), (NC * TOK, 128)
    c_of = iota(shape, 0) // TOK
    blocks = []
    for i in range(CW // 128):
        block = jnp.broadcast_to(values[i : i + 1, :], shape)
        for c in range(1, NC):
            row = c * (CW // 128) + i
            block = jnp.where(c_of == c, jnp.broadcast_to(values[row : row + 1, :], shape), block)
        blocks.append(block)
    return jnp.concatenate(blocks, axis=1)


def minus_expm1(x):
    small = jnp.full_like(x, 1.0)
    for k in range(8, 1, -1):
        small = 1.0 + small * x * (1.0 / k)
    return jnp.where(x > -0.3, -x * small, 1.0 - jnp.exp(x))


def kernel(
    tokens_hbm, gain1_hbm, ids_hbm, weights_hbm, rec_hbm, conv_hbm, logit_hbm, rgain_hbm, gain2_hbm, taps_hbm,
    pin_hbm, pgate_hbm, bdec_hbm, binp_hbm, pout_hbm, eg_hbm, eu_hbm, ed_hbm,
    result_ref, state_ref, newconv_ref,
    tokens_ref, gain1_ref, ids_ref, weights_ref, rec_ref, conv_ref, logit_ref, rgain_ref, gain2_ref, taps_ref,
    wcat, w4, bdec, binp, wgu, wdown,
    tok_s, g1, pb, rp, sb, rb, ob, ib, xg, part, rpart, sums, rright, rleft, ob2, ib2, rw_s,
    lsem, s1, r1, s2p, r2p, s2, r2, s3, r3, s4, r4, s4d, r4d, s5p, r5p, s5, r5r, r5l, s6, r6,
):
    ep = lax.axis_index("ep")
    tp = lax.axis_index("tp")
    z = tp // 2
    core = tp % 2
    other = 1 - core
    mate = (ep, z * 2 + other)

    def along(d):
        return (z + d + NZ) % NZ

    def at_z(zz):
        return (ep, zz * 2 + core)

    barrier = pltpu.get_barrier_semaphore()
    pl.semaphore_signal(barrier, inc=1, device_id=mate, device_id_type=MESH)
    for d in range(1, NZ):
        pl.semaphore_signal(barrier, inc=1, device_id=at_z(along(d)), device_id_type=MESH)
    for d in range(1, NE):
        pl.semaphore_signal(barrier, inc=1, device_id=((ep + d) % NE, tp), device_id_type=MESH)

    smalls = [
        pltpu.make_async_copy(src, dst, lsem.at[11 + i])
        for i, (src, dst) in enumerate((
            (tokens_hbm, tokens_ref), (gain1_hbm, gain1_ref), (ids_hbm, ids_ref), (weights_hbm, weights_ref),
            (rec_hbm, rec_ref), (conv_hbm, conv_ref), (logit_hbm, logit_ref), (rgain_hbm, rgain_ref),
            (gain2_hbm, gain2_ref), (taps_hbm.at[:, pl.ds(pl.multiple_of(tp * W, W), W)], taps_ref),
        ))
    ]
    for load in smalls:
        load.start()
    loads = [
        pltpu.make_async_copy(pin_hbm, wcat.at[:, pl.ds(0, W)], lsem.at[0]),
        pltpu.make_async_copy(pgate_hbm, wcat.at[:, pl.ds(W, W)], lsem.at[1]),
        pltpu.make_async_copy(bdec_hbm.at[tp], bdec, lsem.at[2]),
        pltpu.make_async_copy(binp_hbm.at[tp], binp, lsem.at[3]),
    ]
    for c in range(NC):
        loads.append(
            pltpu.make_async_copy(
                pout_hbm.at[:, pl.ds(c * CW, CW)], w4.at[pl.ds(c * W, W), :], lsem.at[4 + c]
            )
        )
    loads.append(pltpu.make_async_copy(eg_hbm.at[0], wgu.at[:, pl.ds(0, FW)], lsem.at[8]))
    loads.append(pltpu.make_async_copy(eu_hbm.at[0], wgu.at[:, pl.ds(FW, FW)], lsem.at[9]))
    loads.append(pltpu.make_async_copy(ed_hbm.at[0], wdown, lsem.at[10]))
    for load in loads:
        load.start()

    smalls[0].wait()
    smalls[1].wait()
    own = tokens_ref[...].astype(F32)
    for c in range(NC):
        tok_s[c * TOK : (c + 1) * TOK, :] = own[:, c * CW : (c + 1) * CW]
    values = tok_s[...]
    scale = lax.rsqrt(per_token(values * values) * (1.0 / D) + EPS)
    g1[tp] = (values * scale * spread(gain1_ref)).astype(BF16)

    pl.semaphore_wait(barrier, NZ + NE - 1)

    def copy1(dev, slot):
        return pltpu.make_async_remote_copy(
            src_ref=g1.at[slot], dst_ref=g1.at[slot], send_sem=s1, recv_sem=r1.at[slot], device_id=dev, device_id_type=MESH
        )

    for d in (4, 3, 5, 2, 6, 1, 7):
        copy1(at_z(along(d)), tp).start()
    copy1(mate, tp).start()

    q4, r4e = (NC * TOK, W), 8
    row_n, row_c = iota(q4, 0) % TOK, iota(q4, 0) // TOK
    lane_e, lane_c, lane_s = iota(q4, 1) // r4e, (iota(q4, 1) // SLOTS) % NC, iota(q4, 1) % SLOTS
    pick_own = onehot(iota((NC * TOK, NE * TOK), 1) == tp * TOK + iota((NC * TOK, NE * TOK), 0) % TOK)
    smalls[2].wait()
    smalls[3].wait()
    all_ids = ids_ref[...].astype(F32).astype(BF16)
    own_ids = lax.dot_general(pick_own.astype(BF16), all_ids, (((1,), (1,)), ((), ())), preferred_element_type=F32)
    for c in range(NC):
        rw_s[c * TOK : (c + 1) * TOK, :] = weights_ref[...]
    hit = jnp.zeros(q4, F32)
    weighed = jnp.zeros(q4, F32)
    lane_ef = lane_e.astype(F32)
    for k in range(4):
        same = onehot(own_ids[:, k : k + 1] == lane_ef)
        hit = hit + same
        weighed = weighed + same * rw_s[:, k : k + 1]
    sq = (NC * TOK, NC * TOK)
    earlier = onehot(
        (iota(sq, 0) // TOK == iota(sq, 1) // TOK) & (iota(sq, 1) % TOK < iota(sq, 0) % TOK)
    )
    before = dot(earlier.astype(BF16), hit.astype(BF16))
    chosen = hit * onehot((before == lane_s.astype(F32)) & (row_c == lane_c))
    combine = chosen * weighed

    for d in (1, 7, 2, 6, 3, 5, 4):
        slot = along(d) * 2 + core
        copy1(mate, slot).wait_recv()
        copy1(mate, slot).start()
    for d in range(NZ):
        copy1(mate, along(d) * 2 + other).wait_recv()

    big = NT * NC * TOK
    pr, pc = iota((big, big), 0), iota((big, big), 1)
    perm = onehot(pc == ((pr // TOK) % NT) * 16 + (pr // 64) * TOK + pr % TOK).astype(BF16)
    stacked = dot(perm, g1[...].reshape(big, CW)).astype(BF16)
    for load in loads[0:4] + smalls[4:]:
        load.wait()
    both = jnp.zeros((NT * TOK, 2 * W), F32)
    for c in range(NC):
        both = both + dot(stacked[c * 64 : (c + 1) * 64, :], wcat[c * CW : (c + 1) * CW, :])
    joined = both.astype(BF16)
    branch_in, branch_gate = joined[:, :W].astype(F32), joined[:, W:].astype(F32)

    taps = taps_ref[...].astype(F32)
    conv = taps[3:4, :] * branch_in
    for tap in range(3):
        conv = conv + taps[tap : tap + 1, :] * conv_ref[tap].astype(F32)
    newconv_ref[0:2] = conv_ref[1:3]
    newconv_ref[2] = joined[:, :W]

    low = conv.astype(BF16)
    decay_gate = jax.nn.sigmoid(dot(low, bdec[...]))
    input_gate = jax.nn.sigmoid(dot(low, binp[...]))
    mine = iota((NT, W), 0) == tp
    logit = jnp.sum(jnp.where(mine, logit_ref[...], 0.0), axis=0, keepdims=True)
    rgain = jnp.sum(jnp.where(mine, rgain_ref[...].astype(F32), 0.0), axis=0, keepdims=True)
    soft = jnp.maximum(-logit, 0.0) + jnp.log1p(jnp.exp(-jnp.abs(logit)))
    log_keep = -RATE * decay_gate * soft
    new_state = jnp.exp(log_keep) * rec_ref[...] + jnp.sqrt(minus_expm1(2.0 * log_keep)) * input_gate * conv
    state_ref[...] = new_state
    hidden = new_state * jax.nn.gelu(branch_gate)
    squares = jnp.broadcast_to(jnp.sum(hidden * hidden, axis=1, keepdims=True), (NT * TOK, W))

    er, et = iota((big, NT * TOK), 0), iota((big, NT * TOK), 1)
    expand = onehot(et == (((er // 16) % NZ) * 2 + er // 128) * TOK + er % TOK).astype(BF16)
    wide = dot(expand, jnp.concatenate([(hidden * rgain).astype(BF16), squares.astype(BF16)], axis=1))
    gained, sq_wide = wide[:, :W], wide[:, W:]
    c_of = (iota((big, W), 0) // TOK) % NC
    for load in loads[4:8]:
        load.wait()
    lhs = jnp.concatenate([jnp.where(c_of == c, gained, 0.0) for c in range(NC)], axis=1).astype(BF16)
    pb[:, :, :, 0:CW] = dot(lhs, w4[...]).astype(BF16).reshape(2, NZ, 16, CW)
    pb[:, :, :, CW : CW + TAIL] = sq_wide.astype(BF16).reshape(2, NZ, 16, TAIL)

    pair2 = pltpu.make_async_remote_copy(
        src_ref=pb.at[other], dst_ref=rp, send_sem=s2p, recv_sem=r2p, device_id=mate, device_id_type=MESH
    )
    pair2.start()
    pair2.wait_recv()

    def copy2(dev, slot):
        return pltpu.make_async_remote_copy(
            src_ref=sb.at[slot], dst_ref=rb.at[z], send_sem=s2, recv_sem=r2, device_id=dev, device_id_type=MESH
        )

    for d in (4, 3, 5, 2, 6, 1, 7):
        zz = along(d)
        sb[zz] = (pb[core, zz].astype(F32) + rp[zz].astype(F32)).astype(BF16)
        copy2(at_z(zz), zz).start()
    rb[z] = (pb[core, z].astype(F32) + rp[z].astype(F32)).astype(BF16)
    pltpu.make_async_copy(sb.at[pl.ds(0, NZ - 1)], rb.at[pl.ds(0, NZ - 1)], r2).wait()
    summed = jnp.zeros((16, CW + TAIL), F32)
    for zz in range(NZ):
        summed = summed + rb[zz].astype(F32)
    residual = tok_s[...] + summed[:, :CW] * lax.rsqrt(summed[:, CW : CW + 1] * (1.0 / D_REC) + EPS)
    scale = lax.rsqrt(per_token(residual * residual) * (1.0 / D) + EPS)
    second = (residual * scale * spread(gain2_ref)).astype(BF16)
    tok_s[...] = residual

    sent = lax.dot_general(chosen.astype(BF16), second, (((0,), (0,)), ((), ())), preferred_element_type=F32)
    ob[...] = sent.reshape(NE, 8, CW).astype(BF16)
    ib[ep] = ob[ep]

    def copy3(e, src, dst, ss, rs):
        return pltpu.make_async_remote_copy(
            src_ref=src.at[e], dst_ref=dst.at[ep], send_sem=ss, recv_sem=rs, device_id=(e, tp), device_id_type=MESH
        )

    far = (10, 6, 14, 9, 11, 5, 7, 13, 15, 2, 8, 1, 3, 4, 12)
    for d in far:
        copy3((ep + d) % NE, ob, ib, s3, r3).start()
    for load in loads[8:]:
        load.wait()
    pltpu.make_async_copy(ob.at[pl.ds(0, NE - 1)], ib.at[pl.ds(0, NE - 1)], r3).wait()
    own_rows = NE * 8
    sr, sc = iota((own_rows, own_rows), 0), iota((own_rows, own_rows), 1)
    turn = onehot(sc == ((sr // SLOTS) % NE) * 8 + (sr // ROWS) * SLOTS + sr % SLOTS).astype(BF16)
    turned = dot(turn, ib[...].astype(F32).reshape(own_rows, CW).astype(BF16)).astype(BF16)
    for c in range(NC):
        xg[z, core, :, c * CW : (c + 1) * CW] = turned[c * ROWS : (c + 1) * ROWS, :]

    def copy4(zz, h, dev):
        block = xg.at[zz, core, pl.ds(h * HALF, HALF), :]
        return pltpu.make_async_remote_copy(
            src_ref=block, dst_ref=block, send_sem=s4, recv_sem=r4.at[zz * 2 + h], device_id=dev, device_id_type=MESH
        )

    def cross4(zz, h, side):
        block = xg.at[zz, side, pl.ds(h * HALF, HALF), :]
        return pltpu.make_async_remote_copy(
            src_ref=block, dst_ref=block, send_sem=s4d, recv_sem=r4d.at[zz * 2 + h], device_id=mate, device_id_type=MESH
        )

    right, left = at_z(along(1)), at_z(along(-1))
    for h in range(2):
        copy4(z, h, right).start()
        copy4(z, 1 - h, left).start()
    cross4(z, 0, core).start()
    cross4(z, 1, core).start()

    def run_expert(zz):
        for h in range(2):
            cross4(zz, h, other).wait_recv()
        rows = xg[zz].reshape(2 * ROWS, D)
        gu = dot(rows, wgu[...])
        gate, up = jnp.minimum(gu[:, :FW], CLAMP), jnp.clip(gu[:, FW:], -CLAMP, CLAMP)
        act = ((up + 1.0) * (gate * jax.nn.sigmoid(ALPHA * gate))).astype(BF16)
        part[zz] = dot(act, wdown[...]).astype(BF16).reshape(2, ROWS, D)
        pltpu.make_async_remote_copy(
            src_ref=part.at[zz, other], dst_ref=rpart.at[zz], send_sem=s5p, recv_sem=r5p.at[zz], device_id=mate, device_id_type=MESH
        ).start()

    for s in range(1, 5):
        for i in range(2):
            for h, way, hops, nxt in ((i, -1, 4 - i, right), (1 - i, 1, 4 - i, left)):
                if s <= hops:
                    zz = along(way * s)
                    copy4(zz, h, nxt).wait_recv()
                    if s < hops:
                        copy4(zz, h, nxt).start()
                    cross4(zz, h, core).start()
        if s == 1:
            run_expert(z)
        else:
            pl.loop(0, 2)(lambda i, s=s: run_expert(along((s - 1) * (1 - 2 * i))))
    def pair_sum(zz, h):
        rows = slice(h * HALF, (h + 1) * HALF)
        return part[zz, core, rows, :].astype(F32) + rpart[zz, rows, :].astype(F32)

    def wait_pair(zz):
        pltpu.make_async_remote_copy(
            src_ref=part.at[zz, other], dst_ref=rpart.at[zz], send_sem=s5p, recv_sem=r5p.at[zz], device_id=mate, device_id_type=MESH
        ).wait_recv()

    def copy5(zz, h, hop, to_right):
        return pltpu.make_async_remote_copy(
            src_ref=sums.at[zz, h],
            dst_ref=(rright if to_right else rleft).at[h, hop],
            send_sem=s5,
            recv_sem=(r5r if to_right else r5l).at[h * 4 + hop],
            device_id=right if to_right else left,
            device_id_type=MESH,
        )

    def got5(h, hop, from_left):
        return (rright if from_left else rleft)[h, hop].astype(F32)

    def pass_on(hop, h, to_right):
        zz = along(hop if to_right else -hop)
        total = pair_sum(zz, h)
        if hop < (4 - h if to_right else 3 + h):
            copy5(zz, h, hop, to_right).wait_recv()
            total = total + got5(h, hop, to_right)
        sums[zz, h] = total.astype(BF16)
        copy5(zz, h, hop - 1, to_right).start()

    wait_pair(along(3))
    pass_on(3, 1, True)
    wait_pair(along(-3))
    pass_on(3, 0, False)
    run_expert(along(4))
    wait_pair(along(2))
    wait_pair(along(-2))
    wait_pair(along(4))
    pass_on(4, 0, True)
    pass_on(4, 1, False)
    for hop in (2, 1):
        pass_on(hop, 1, True)
        pass_on(hop, 0, False)
        if hop == 2:
            wait_pair(along(1))
            wait_pair(along(-1))
        pass_on(hop + 1, 0, True)
        pass_on(hop + 1, 1, False)
    pass_on(1, 0, True)
    pass_on(1, 1, False)
    wait_pair(z)
    for h in range(2):
        total = pair_sum(z, h)
        for to_right in (True, False):
            copy5(z, h, 0, to_right).wait_recv()
            total = total + got5(h, 0, to_right)
        sums[z, h] = total.astype(BF16)

    mine = jnp.concatenate([sums[z].reshape(ROWS, D)[:, c * CW : (c + 1) * CW] for c in range(NC)], axis=0)
    back = onehot(sr == ((sc // SLOTS) % NE) * 8 + (sc // ROWS) * SLOTS + sc % SLOTS).astype(BF16)
    ob2[...] = dot(back, mine).reshape(NE, 8, CW).astype(BF16)
    ib2[ep] = ob2[ep]
    for d in far:
        copy3((ep + d) % NE, ob2, ib2, s6, r6).start()
    high = combine.astype(BF16)
    rest = combine - high.astype(F32)
    middle = rest.astype(BF16)
    lowest = (rest - middle.astype(F32)).astype(BF16)
    pltpu.make_async_copy(ob2.at[pl.ds(0, NE - 1)], ib2.at[pl.ds(0, NE - 1)], r6).wait()
    returned = ib2[...].astype(F32).reshape(NE * 8, CW).astype(BF16)
    mix = dot(lowest, returned) + dot(middle, returned) + dot(high, returned)
    tok_s[...] = tok_s[...] + mix
    for c in range(NC):
        result_ref[:, c * CW : (c + 1) * CW] = tok_s[c * TOK : (c + 1) * TOK, :].astype(BF16)

    def drain(ref, sem):
        pltpu.make_async_copy(ref, ref, sem).wait()

    drain(g1.at[pl.ds(0, NT - 1)], s1)
    pair2.wait_send()
    drain(sb.at[pl.ds(0, NZ - 1)], s2)
    drain(ob.at[pl.ds(0, NE - 1)], s3)
    drain(xg.at[pl.ds(0, NZ - 1), 0], s4)
    drain(xg.at[:, 0], s4d)
    drain(rpart, s5p)
    drain(sums.at[pl.ds(0, NZ - 1)], s5)
    drain(ob2.at[pl.ds(0, NE - 1)], s6)


def per_device(
    tokens, rec_state, conv_state, route_ids, route_weights, first_gain, proj_input, proj_gate, conv_taps,
    decay_logit, block_decay, block_input, rec_gain, proj_out, second_gain, expert_gate, expert_up, expert_down,
):
    seqs = rec_state.shape[0]
    vmem, hbm = pl.BlockSpec(memory_space=pltpu.VMEM), pl.BlockSpec(memory_space=pl.ANY)
    dma, v = pltpu.SemaphoreType.DMA, pltpu.VMEM
    result, new_state, new_conv = pl.pallas_call(
        kernel,
        name="layer",
        out_shape=(v(tokens.shape, BF16), v(rec_state.shape, F32), v((3, seqs, W), BF16)),
        in_specs=[hbm] * 18,
        out_specs=(vmem, vmem, vmem),
        scratch_shapes=[
            v(tokens.shape, BF16), v((D // W, W), BF16), v((TOK, seqs), I32), v((TOK, TOK), F32),
            v((seqs, W), F32), v((3, seqs, W), BF16), v((NT, W), F32), v((NT, W), BF16), v((D // W, W), BF16), v((TOK, W), BF16),
            v((D, 2 * W), BF16), v((NC * W, CW), BF16), v((W, W), BF16), v((W, W), BF16),
            v((D, 2 * FW), BF16), v((FW, D), BF16),
            v((16, CW), F32), v((NT, 16, CW), BF16),
            v((2, NZ, 16, CW + TAIL), BF16), v((NZ, 16, CW + TAIL), BF16), v((NZ, 16, CW + TAIL), BF16),
            v((NZ, 16, CW + TAIL), BF16),
            v((NE, 8, CW), BF16), v((NE, 8, CW), BF16),
            v((NZ, 2, ROWS, D), BF16), v((NZ, 2, ROWS, D), BF16), v((NZ, ROWS, D), BF16),
            v((NZ, 2, HALF, D), BF16), v((2, 4, HALF, D), BF16), v((2, 4, HALF, D), BF16),
            v((NE, 8, CW), BF16), v((NE, 8, CW), BF16), v((16, 4), F32),
            dma((21,)), dma, dma((NT,)), dma, dma, dma, dma, dma, dma,
            dma, dma((NZ * 2,)), dma, dma((NZ * 2,)), dma, dma((NZ,)), dma, dma((8,)), dma((8,)), dma, dma,
        ],
        compiler_params=pltpu.CompilerParams(
            collective_id=0, has_side_effects=True, vmem_limit_bytes=60 * 1024 * 1024
        ),
    )(
        tokens, first_gain.reshape(D // W, W), route_ids.T, route_weights, rec_state, conv_state.transpose(1, 0, 2),
        decay_logit.reshape(NT, W), rec_gain.reshape(NT, W), second_gain.reshape(D // W, W), conv_taps,
        proj_input, proj_gate, block_decay, block_input, proj_out, expert_gate, expert_up, expert_down,
    )
    return result, new_state, new_conv.transpose(1, 0, 2)


def solution(mesh):
    in_specs = (
        P(("ep", "tp"), None),
        P("ep", "tp"),
        P("ep", None, "tp"),
        P("ep", None),
        P(("ep", "tp"), None),
        P(),
        P(None, "tp"),
        P(None, "tp"),
        P(),
        P(),
        P(),
        P(),
        P(),
        P("tp", None),
        P(),
        P("ep", None, "tp"),
        P("ep", None, "tp"),
        P("ep", "tp", None),
    )
    out_specs = (P(("ep", "tp"), None), P("ep", "tp"), P("ep", None, "tp"))
    return jax.shard_map(
        per_device, mesh=mesh, in_specs=in_specs, out_specs=out_specs, check_vma=False
    )
```

```python
import jax
import jax.numpy as jnp
from jax import lax
from jax.experimental import pallas as pl
from jax.experimental.pallas import tpu as pltpu
from jax.sharding import PartitionSpec as P

MESH = pl.DeviceIdType.MESH
BF16, F32, I32 = jnp.bfloat16, jnp.float32, jnp.int32

EPS = 1e-06
CLAMP = 7.0
ALPHA = 1.702
RATE = 8.0

D = 4096
NC = 4
CW = D // NC
TOK = 4
NE = 16
NT = 16
NZ = 8
D_REC = 2048
W = 128
FW = 256
SLOTS = 2
ROWS = NE * SLOTS
HALF = ROWS // 2
TAIL = 128
CB = 384
CA = CW - CB
DA, DB = NC * CA, NC * CB


def iota(shape, dim):
    return lax.broadcasted_iota(I32, shape, dim)


def onehot(cond):
    return jnp.where(cond, 1.0, 0.0).astype(F32)


def dot(a, b):
    return jnp.dot(a, b, preferred_element_type=F32)


def per_token(values):
    part = jnp.broadcast_to(jnp.sum(values, axis=1, keepdims=True), (NC * TOK, 128))
    total = part
    for c in range(1, NC):
        total = total + pltpu.roll(part, c * TOK, 0)
    return total[:, 0:1]


def spread(ref):
    values, shape = ref[...].astype(F32), (NC * TOK, 128)
    c_of = iota(shape, 0) // TOK
    blocks = []
    for i in range(CW // 128):
        block = jnp.broadcast_to(values[i : i + 1, :], shape)
        for c in range(1, NC):
            row = c * (CW // 128) + i
            block = jnp.where(c_of == c, jnp.broadcast_to(values[row : row + 1, :], shape), block)
        blocks.append(block)
    return jnp.concatenate(blocks, axis=1)


def minus_expm1(x):
    small = jnp.full_like(x, 1.0)
    for k in range(8, 1, -1):
        small = 1.0 + small * x * (1.0 / k)
    return jnp.where(x > -0.3, -x * small, 1.0 - jnp.exp(x))


def kernel(
    tokens_hbm, gain1_hbm, ids_hbm, weights_hbm, rec_hbm, conv_hbm, logit_hbm, rgain_hbm, gain2_hbm, taps_hbm,
    pin_hbm, pgate_hbm, bdec_hbm, binp_hbm, pout_hbm, eg_hbm, eu_hbm, ed_hbm,
    result_ref, state_ref, newconv_ref,
    tokens_ref, gain1_ref, ids_ref, weights_ref, rec_ref, conv_ref, logit_ref, rgain_ref, gain2_ref, taps_ref,
    wcat, w4, bdec, binp, wgu_a, wgu_b, wdown_a, wdown_b,
    tok_s, g1, pb, rp, sb, rb, ob, ib, xa, acc, part_a, rpart_a, sums, rright, rleft, ob2, ib2, rw_s,
    sg, tb, xr, xb, part_b, rpart_b, tb2, rr, cb, rcb,
    lsem, s1, r1, s2p, r2p, s2, r2, s3, r3, s4, r4, s4d, r4d, s5p, r5p, s5, r5r, r5l, s6, r6,
    sb1, rb1, sb2, rb2, sb2d, rb2d, sbp, rbp, sb3, rb3, sb4, rb4,
):
    ep = lax.axis_index("ep")
    tp = lax.axis_index("tp")
    z = tp // 2
    core = tp % 2
    other = 1 - core
    mate = (ep, z * 2 + other)
    y, x = ep // 4, ep % 4

    def remote(src, dst, ss, rs, dev):
        return pltpu.make_async_remote_copy(
            src_ref=src, dst_ref=dst, send_sem=ss, recv_sem=rs, device_id=dev, device_id_type=MESH
        )

    def over(dy, dx):
        return ((y + dy + 4) % 4) * 4 + (x + dx + 4) % 4

    def along(d):
        return (z + d + NZ) % NZ

    def at_z(zz):
        return (ep, zz * 2 + core)

    barrier = pltpu.get_barrier_semaphore()
    pl.semaphore_signal(barrier, inc=1, device_id=mate, device_id_type=MESH)
    for d in range(1, NZ):
        pl.semaphore_signal(barrier, inc=1, device_id=at_z(along(d)), device_id_type=MESH)
    for d in range(1, NE):
        pl.semaphore_signal(barrier, inc=1, device_id=((ep + d) % NE, tp), device_id_type=MESH)

    smalls = [
        pltpu.make_async_copy(src, dst, lsem.at[11 + i])
        for i, (src, dst) in enumerate((
            (tokens_hbm, tokens_ref), (gain1_hbm, gain1_ref), (ids_hbm, ids_ref), (weights_hbm, weights_ref),
            (rec_hbm, rec_ref), (conv_hbm, conv_ref), (logit_hbm, logit_ref), (rgain_hbm, rgain_ref),
            (gain2_hbm, gain2_ref), (taps_hbm.at[:, pl.ds(pl.multiple_of(tp * W, W), W)], taps_ref),
        ))
    ]
    for load in smalls:
        load.start()
    loads = [
        pltpu.make_async_copy(pin_hbm, wcat.at[:, pl.ds(0, W)], lsem.at[0]),
        pltpu.make_async_copy(pgate_hbm, wcat.at[:, pl.ds(W, W)], lsem.at[1]),
        pltpu.make_async_copy(bdec_hbm.at[tp], bdec, lsem.at[2]),
        pltpu.make_async_copy(binp_hbm.at[tp], binp, lsem.at[3]),
    ]
    for c in range(NC):
        loads.append(
            pltpu.make_async_copy(
                pout_hbm.at[:, pl.ds(c * CW, CW)], w4.at[pl.ds(c * W, W), :], lsem.at[4 + c]
            )
        )
    for load in loads:
        load.start()
    for c in range(NC):
        for i, (hbm, col) in enumerate(((eg_hbm, 0), (eu_hbm, FW))):
            for dst, first, size, sem in ((wgu_a, 0, CA, 8), (wgu_b, CA, CB, 9)):
                pltpu.make_async_copy(
                    hbm.at[0, pl.ds(c * CW + first, size), :],
                    dst.at[pl.ds(c * size, size), pl.ds(col, FW)],
                    lsem.at[sem],
                ).start()
        for dst, first, size, sem in ((wdown_a, 0, CA, 10), (wdown_b, CA, CB, 21)):
            pltpu.make_async_copy(
                ed_hbm.at[0, :, pl.ds(c * CW + first, size)], dst.at[:, pl.ds(c * size, size)], lsem.at[sem]
            ).start()

    smalls[0].wait()
    smalls[1].wait()
    own = tokens_ref[...].astype(F32)
    for c in range(NC):
        tok_s[c * TOK : (c + 1) * TOK, :] = own[:, c * CW : (c + 1) * CW]
    values = tok_s[...]
    scale = lax.rsqrt(per_token(values * values) * (1.0 / D) + EPS)
    g1[tp] = (values * scale * spread(gain1_ref)).astype(BF16)

    pl.semaphore_wait(barrier, NZ + NE - 1)

    def copy1(dev, slot):
        return pltpu.make_async_remote_copy(
            src_ref=g1.at[slot], dst_ref=g1.at[slot], send_sem=s1, recv_sem=r1.at[slot], device_id=dev, device_id_type=MESH
        )

    for d in (4, 3, 5, 2, 6, 1, 7):
        copy1(at_z(along(d)), tp).start()
    copy1(mate, tp).start()

    q4, r4e = (NC * TOK, W), 8
    row_n, row_c = iota(q4, 0) % TOK, iota(q4, 0) // TOK
    lane_e, lane_c, lane_s = iota(q4, 1) // r4e, (iota(q4, 1) // SLOTS) % NC, iota(q4, 1) % SLOTS
    pick_own = onehot(iota((NC * TOK, NE * TOK), 1) == tp * TOK + iota((NC * TOK, NE * TOK), 0) % TOK)
    smalls[2].wait()
    smalls[3].wait()
    all_ids = ids_ref[...].astype(F32).astype(BF16)
    own_ids = lax.dot_general(pick_own.astype(BF16), all_ids, (((1,), (1,)), ((), ())), preferred_element_type=F32)
    for c in range(NC):
        rw_s[c * TOK : (c + 1) * TOK, :] = weights_ref[...]
    hit = jnp.zeros(q4, F32)
    weighed = jnp.zeros(q4, F32)
    lane_ef = lane_e.astype(F32)
    for k in range(4):
        same = onehot(own_ids[:, k : k + 1] == lane_ef)
        hit = hit + same
        weighed = weighed + same * rw_s[:, k : k + 1]
    sq = (NC * TOK, NC * TOK)
    earlier = onehot(
        (iota(sq, 0) // TOK == iota(sq, 1) // TOK) & (iota(sq, 1) % TOK < iota(sq, 0) % TOK)
    )
    before = dot(earlier.astype(BF16), hit.astype(BF16))
    chosen = hit * onehot((before == lane_s.astype(F32)) & (row_c == lane_c))
    combine = chosen * weighed

    qn, rn = NZ * NC * TOK, NE * NZ * SLOTS
    big_q = (qn, rn)
    pick_core = onehot(
        iota((qn, NE * TOK), 1) == ((iota((qn, NE * TOK), 0) // 16) * 2 + core) * TOK + iota((qn, NE * TOK), 0) % TOK
    )
    core_ids = lax.dot_general(pick_core.astype(BF16), all_ids, (((1,), (1,)), ((), ())), preferred_element_type=F32)
    big_e = (iota(big_q, 1) // (NZ * SLOTS)).astype(F32)
    big_s = (iota(big_q, 1) % SLOTS).astype(F32)
    same_z = iota(big_q, 0) // 16 == (iota(big_q, 1) // SLOTS) % NZ
    big_hit = jnp.zeros(big_q, F32)
    for k in range(4):
        big_hit = big_hit + onehot(core_ids[:, k : k + 1] == big_e)
    qq = (qn, qn)
    big_earlier = onehot(
        (iota(qq, 0) // TOK == iota(qq, 1) // TOK) & (iota(qq, 1) % TOK < iota(qq, 0) % TOK)
    )
    big_before = dot(big_earlier.astype(BF16), big_hit.astype(BF16))
    big_chosen = big_hit * onehot((big_before == big_s) & same_z)
    c_of_q = (iota(big_q, 0) // TOK) % NC

    for d in (1, 7, 2, 6, 3, 5, 4):
        slot = along(d) * 2 + core
        copy1(mate, slot).wait_recv()
        copy1(mate, slot).start()
    for d in range(NZ):
        copy1(mate, along(d) * 2 + other).wait_recv()

    big = NT * NC * TOK
    pr, pc = iota((big, big), 0), iota((big, big), 1)
    perm = onehot(pc == ((pr // TOK) % NT) * 16 + (pr // 64) * TOK + pr % TOK).astype(BF16)
    stacked = dot(perm, g1[...].reshape(big, CW)).astype(BF16)
    for load in loads[0:4] + smalls[4:]:
        load.wait()
    both = jnp.zeros((NT * TOK, 2 * W), F32)
    for c in range(NC):
        both = both + dot(stacked[c * 64 : (c + 1) * 64, :], wcat[c * CW : (c + 1) * CW, :])
    joined = both.astype(BF16)
    branch_in, branch_gate = joined[:, :W].astype(F32), joined[:, W:].astype(F32)

    taps = taps_ref[...].astype(F32)
    conv = taps[3:4, :] * branch_in
    for tap in range(3):
        conv = conv + taps[tap : tap + 1, :] * conv_ref[tap].astype(F32)
    newconv_ref[0:2] = conv_ref[1:3]
    newconv_ref[2] = joined[:, :W]

    low = conv.astype(BF16)
    decay_gate = jax.nn.sigmoid(dot(low, bdec[...]))
    input_gate = jax.nn.sigmoid(dot(low, binp[...]))
    mine = iota((NT, W), 0) == tp
    logit = jnp.sum(jnp.where(mine, logit_ref[...], 0.0), axis=0, keepdims=True)
    rgain = jnp.sum(jnp.where(mine, rgain_ref[...].astype(F32), 0.0), axis=0, keepdims=True)
    soft = jnp.maximum(-logit, 0.0) + jnp.log1p(jnp.exp(-jnp.abs(logit)))
    log_keep = -RATE * decay_gate * soft
    new_state = jnp.exp(log_keep) * rec_ref[...] + jnp.sqrt(minus_expm1(2.0 * log_keep)) * input_gate * conv
    state_ref[...] = new_state
    hidden = new_state * jax.nn.gelu(branch_gate)
    squares = jnp.broadcast_to(jnp.sum(hidden * hidden, axis=1, keepdims=True), (NT * TOK, W))

    er, et = iota((big, NT * TOK), 0), iota((big, NT * TOK), 1)
    expand = onehot(et == (((er // 16) % NZ) * 2 + er // 128) * TOK + er % TOK).astype(BF16)
    wide = dot(expand, jnp.concatenate([(hidden * rgain).astype(BF16), squares.astype(BF16)], axis=1))
    gained, sq_wide = wide[:, :W], wide[:, W:]
    c_of = (iota((big, W), 0) // TOK) % NC
    for load in loads[4:8]:
        load.wait()
    lhs = jnp.concatenate([jnp.where(c_of == c, gained, 0.0) for c in range(NC)], axis=1).astype(BF16)
    pb[:, :, :, 0:CW] = dot(lhs, w4[...]).astype(BF16).reshape(2, NZ, 16, CW)
    pb[:, :, :, CW : CW + TAIL] = sq_wide.astype(BF16).reshape(2, NZ, 16, TAIL)

    pair2 = pltpu.make_async_remote_copy(
        src_ref=pb.at[other], dst_ref=rp, send_sem=s2p, recv_sem=r2p, device_id=mate, device_id_type=MESH
    )
    pair2.start()
    pair2.wait_recv()

    def copy2(dev, slot):
        return pltpu.make_async_remote_copy(
            src_ref=sb.at[slot], dst_ref=rb.at[z], send_sem=s2, recv_sem=r2, device_id=dev, device_id_type=MESH
        )

    for d in (4, 3, 5, 2, 6, 1, 7):
        zz = along(d)
        sb[zz] = (pb[core, zz].astype(F32) + rp[zz].astype(F32)).astype(BF16)
        copy2(at_z(zz), zz).start()
    rb[z] = (pb[core, z].astype(F32) + rp[z].astype(F32)).astype(BF16)
    pltpu.make_async_copy(sb.at[pl.ds(0, NZ - 1)], rb.at[pl.ds(0, NZ - 1)], r2).wait()
    summed = jnp.zeros((16, CW + TAIL), F32)
    for zz in range(NZ):
        summed = summed + rb[zz].astype(F32)
    residual = tok_s[...] + summed[:, :CW] * lax.rsqrt(summed[:, CW : CW + 1] * (1.0 / D_REC) + EPS)
    scale = lax.rsqrt(per_token(residual * residual) * (1.0 / D) + EPS)
    second = (residual * scale * spread(gain2_ref)).astype(BF16)
    tok_s[...] = residual

    w_high = rw_s[...].astype(BF16).astype(F32)
    w_rest = rw_s[...] - w_high
    lane = iota((NC * TOK, TAIL), 1)
    tail = jnp.zeros((NC * TOK, TAIL), F32)
    for k in range(4):
        tail = jnp.where(lane == k, w_high[:, k : k + 1], tail)
        tail = jnp.where(lane == 4 + k, w_rest[:, k : k + 1], tail)
    sg[z, :, 0:CB] = second[:, CA:]
    sg[z, :, CB:] = tail.astype(BF16)
    sent = lax.dot_general(
        chosen.astype(BF16), second[:, :CA], (((0,), (0,)), ((), ())), preferred_element_type=F32
    )
    ob[...] = sent.reshape(NE, 8, CA).astype(BF16)
    ib[ep] = ob[ep]
    for d in (4, 3, 5, 2, 6, 1, 7):
        remote(sg.at[z], sg.at[z], sb1, rb1, at_z(along(d))).start()

    ways = (
        (2, 2), (2, 1), (1, 3), (3, 2), (0, 2), (2, 3), (1, 2), (2, 0),
        (3, 1), (3, 3), (1, 1), (0, 3), (1, 0), (0, 1), (3, 0),
    )

    def to_experts(src, dst, ss, rs):
        for dy, dx in ways:
            e = over(dy, dx)
            remote(src.at[e], dst.at[ep], ss, rs, (e, tp)).start()

    to_experts(ob, ib, s3, r3)

    def all_of(ref, sem):
        pltpu.make_async_copy(ref, ref, sem).wait()

    all_of(ib.at[pl.ds(0, NE - 1)], r3)
    own_rows = NE * 8
    sr, sc = iota((own_rows, own_rows), 0), iota((own_rows, own_rows), 1)
    turn = onehot(sc == ((sr // SLOTS) % NE) * 8 + (sr // ROWS) * SLOTS + sr % SLOTS).astype(BF16)
    turned = dot(turn, ib[...].astype(F32).reshape(own_rows, CA).astype(BF16)).astype(BF16)
    for c in range(NC):
        xa[z, core, :, c * CA : (c + 1) * CA] = turned[c * ROWS : (c + 1) * ROWS, :]

    def copy4(zz, h, dev):
        block = xa.at[zz, core, pl.ds(h * HALF, HALF), :]
        return remote(block, block, s4, r4.at[zz * 2 + h], dev)

    def cross4(zz, h, side):
        block = xa.at[zz, side, pl.ds(h * HALF, HALF), :]
        return remote(block, block, s4d, r4d.at[zz * 2 + h], mate)

    right, left = at_z(along(1)), at_z(along(-1))
    for h in range(2):
        copy4(z, h, right).start()
        copy4(z, 1 - h, left).start()
    cross4(z, 0, core).start()
    cross4(z, 1, core).start()

    all_of(sg.at[pl.ds(0, NZ - 1)], rb1)
    group = sg[...].reshape(qn, CB + TAIL)
    for c in range(NC):
        chosen_c = jnp.where(c_of_q == c, big_chosen, 0.0).astype(BF16)
        picked = lax.dot_general(
            chosen_c, group[:, :CB], (((0,), (0,)), ((), ())), preferred_element_type=F32
        )
        tb[:, :, c * CB : (c + 1) * CB] = picked.reshape(NE, NZ * SLOTS, CB).astype(BF16)
    for dy, dx in ways:
        e = over(dy, dx)
        remote(tb.at[e], xr.at[core, ep], sb2, rb2.at[ep], (e, tp)).start()
    xr[core, ep] = tb[ep]
    remote(tb.at[ep], xr.at[core, ep], sb2d, rb2d, mate).start()

    def across(first, last):
        for dy, dx in ways[first:last]:
            source = over(-dy, -dx)
            block = xr.at[core, source]
            remote(block, block, sb2, rb2.at[source], mate).wait_recv()
            remote(block, block, sb2d, rb2d, mate).start()

    all_of(wgu_a, lsem.at[8])

    def first_part(zz):
        for h in range(2):
            cross4(zz, h, other).wait_recv()
        acc[zz] = dot(xa[zz].reshape(2 * ROWS, DA), wgu_a[...])

    for s in range(1, 5):
        for i in range(2):
            for h, way, hops, nxt in ((i, -1, 4 - i, right), (1 - i, 1, 4 - i, left)):
                if s <= hops:
                    zz = along(way * s)
                    copy4(zz, h, nxt).wait_recv()
                    if s < hops:
                        copy4(zz, h, nxt).start()
                    cross4(zz, h, core).start()
        if s == 1:
            first_part(z)
        else:
            pl.loop(0, 2)(lambda i, s=s: first_part(along((s - 1) * (1 - 2 * i))))
    across(0, len(ways))
    first_part(along(4))

    tr, tc = iota((rn, rn), 0), iota((rn, rn), 1)
    by_z = onehot(tc == ((tr // SLOTS) % NE) * 16 + (tr // ROWS) * SLOTS + tr % SLOTS).astype(BF16)
    all_of(wgu_b, lsem.at[9])
    all_of(wdown_a, lsem.at[10])
    all_of(wdown_b, lsem.at[21])
    xb[:, core] = dot(by_z, xr[core].reshape(rn, DB)).astype(BF16).reshape(NZ, ROWS, DB)
    all_of(xr.at[core], rb2d)
    xb[:, other] = dot(by_z, xr[other].reshape(rn, DB)).astype(BF16).reshape(NZ, ROWS, DB)

    def pair_a(zz):
        return remote(part_a.at[zz, other], rpart_a.at[zz], s5p, r5p.at[zz], mate)

    def finish(one, two):
        rows = jnp.concatenate([xb[one].reshape(2 * ROWS, DB), xb[two].reshape(2 * ROWS, DB)], axis=0)
        gu = jnp.concatenate([acc[one], acc[two]], axis=0) + dot(rows, wgu_b[...])
        gate, up = jnp.minimum(gu[:, :FW], CLAMP), jnp.clip(gu[:, FW:], -CLAMP, CLAMP)
        act = ((up + 1.0) * (gate * jax.nn.sigmoid(ALPHA * gate))).astype(BF16)
        out = dot(act, wdown_a[...]).astype(BF16)
        part_a[one] = out[: 2 * ROWS].reshape(2, ROWS, DA)
        part_a[two] = out[2 * ROWS :].reshape(2, ROWS, DA)
        out = dot(act, wdown_b[...]).astype(BF16)
        for i, zz in enumerate((one, two)):
            for side in range(2):
                at = (2 * i + side) * ROWS
                part_b[side, zz] = out[at : at + ROWS]
        for zz in (one, two):
            pair_a(zz).start()
            remote(part_b.at[other, zz], rpart_b.at[zz], sbp, rbp, mate).start()

    def pair_sum(zz, h):
        rows = slice(h * HALF, (h + 1) * HALF)
        return part_a[zz, core, rows, :].astype(F32) + rpart_a[zz, rows, :].astype(F32)

    def copy5(zz, h, hop, to_right):
        return remote(
            sums.at[zz, h],
            (rright if to_right else rleft).at[h, hop],
            s5,
            (r5r if to_right else r5l).at[h * 4 + hop],
            right if to_right else left,
        )

    def got5(h, hop, from_left):
        return (rright if from_left else rleft)[h, hop].astype(F32)

    def pass_on(hop, h, to_right):
        zz = along(hop if to_right else -hop)
        total = pair_sum(zz, h)
        if hop < (4 - h if to_right else 3 + h):
            copy5(zz, h, hop, to_right).wait_recv()
            total = total + got5(h, hop, to_right)
        sums[zz, h] = total.astype(BF16)
        copy5(zz, h, hop - 1, to_right).start()

    finish(along(3), along(-3))
    finish(along(4), z)
    pair_a(along(3)).wait_recv()
    pass_on(3, 1, True)
    pair_a(along(-3)).wait_recv()
    pass_on(3, 0, False)
    finish(along(2), along(-2))
    pair_a(along(4)).wait_recv()
    pass_on(4, 0, True)
    pass_on(4, 1, False)
    finish(along(1), along(-1))
    pair_a(along(2)).wait_recv()
    pair_a(along(-2)).wait_recv()

    by_a = onehot(tr == ((tc // SLOTS) % NE) * 16 + (tc // ROWS) * SLOTS + tc % SLOTS).astype(BF16)
    half_sum = dot(by_a, part_b[core].reshape(rn, DB))
    all_of(rpart_b, rbp)
    half_sum = half_sum + dot(by_a, rpart_b[...].reshape(rn, DB))
    tb2[...] = half_sum.astype(BF16).reshape(NE, NZ * SLOTS, DB)
    to_experts(tb2, rr, sb3, rb3)
    rr[ep] = tb2[ep]

    for hop in (2, 1):
        pass_on(hop, 1, True)
        pass_on(hop, 0, False)
        if hop == 2:
            pair_a(along(1)).wait_recv()
            pair_a(along(-1)).wait_recv()
        pass_on(hop + 1, 0, True)
        pass_on(hop + 1, 1, False)
    pass_on(1, 0, True)
    pass_on(1, 1, False)
    pair_a(z).wait_recv()
    for h in range(2):
        total = pair_sum(z, h)
        for to_right in (True, False):
            copy5(z, h, 0, to_right).wait_recv()
            total = total + got5(h, 0, to_right)
        sums[z, h] = total.astype(BF16)

    mine = jnp.concatenate([sums[z].reshape(ROWS, DA)[:, c * CA : (c + 1) * CA] for c in range(NC)], axis=0)
    back = onehot(sr == ((sc // SLOTS) % NE) * 8 + (sc // ROWS) * SLOTS + sc % SLOTS).astype(BF16)
    ob2[...] = dot(back, mine).reshape(NE, 8, CA).astype(BF16)
    ib2[ep] = ob2[ep]
    to_experts(ob2, ib2, s6, r6)

    def in_two(values):
        high = values.astype(BF16)
        return high, (values - high.astype(F32)).astype(BF16)

    tails = sg[...].reshape(qn, CB + TAIL)[:, CB:].astype(F32)
    big_weighed = jnp.zeros(big_q, F32)
    for k in range(4):
        weight = tails[:, k : k + 1] + tails[:, 4 + k : 5 + k]
        big_weighed = big_weighed + onehot(core_ids[:, k : k + 1] == big_e) * weight
    big_high, big_low = in_two(big_chosen * big_weighed)
    all_of(rr.at[pl.ds(0, NE - 1)], rb3)
    taken = rr[...].reshape(rn, DB)
    mixed = jnp.zeros((qn, CB), F32)
    for c in range(NC):
        piece = taken[:, c * CB : (c + 1) * CB]
        for factor in (big_low, big_high):
            mixed = mixed + dot(jnp.where(c_of_q == c, factor.astype(F32), 0.0).astype(BF16), piece)
    cb[...] = mixed.astype(BF16).reshape(NZ, 16, CB)
    for d in (4, 3, 5, 2, 6, 1, 7):
        remote(cb.at[along(d)], rcb.at[z], sb4, rb4, at_z(along(d))).start()
    rcb[z] = cb[z]

    high = combine.astype(BF16)
    rest = combine - high.astype(F32)
    middle, lowest = in_two(rest)
    all_of(ib2.at[pl.ds(0, NE - 1)], r6)
    returned = ib2[...].astype(F32).reshape(NE * 8, CA).astype(BF16)
    mix_a = dot(lowest, returned) + dot(middle, returned) + dot(high, returned)
    all_of(rcb.at[pl.ds(0, NZ - 1)], rb4)
    mix_b = jnp.zeros((16, CB), F32)
    for zz in range(NZ):
        mix_b = mix_b + rcb[zz].astype(F32)
    tok_s[:, :CA] = tok_s[:, :CA] + mix_a
    tok_s[:, CA:] = tok_s[:, CA:] + mix_b
    for c in range(NC):
        result_ref[:, c * CW : (c + 1) * CW] = tok_s[c * TOK : (c + 1) * TOK, :].astype(BF16)

    all_of(g1.at[pl.ds(0, NT - 1)], s1)
    pair2.wait_send()
    all_of(sb.at[pl.ds(0, NZ - 1)], s2)
    all_of(ob.at[pl.ds(0, NE - 1)], s3)
    all_of(xa.at[pl.ds(0, NZ - 1), 0], s4)
    all_of(xa.at[:, 0], s4d)
    all_of(rpart_a, s5p)
    all_of(sums.at[pl.ds(0, NZ - 1)], s5)
    all_of(ob2.at[pl.ds(0, NE - 1)], s6)
    all_of(sg.at[pl.ds(0, NZ - 1)], sb1)
    all_of(tb.at[pl.ds(0, NE - 1)], sb2)
    all_of(tb, sb2d)
    all_of(rpart_b, sbp)
    all_of(tb2.at[pl.ds(0, NE - 1)], sb3)
    all_of(cb.at[pl.ds(0, NZ - 1)], sb4)


def per_device(
    tokens, rec_state, conv_state, route_ids, route_weights, first_gain, proj_input, proj_gate, conv_taps,
    decay_logit, block_decay, block_input, rec_gain, proj_out, second_gain, expert_gate, expert_up, expert_down,
):
    seqs = rec_state.shape[0]
    vmem, hbm = pl.BlockSpec(memory_space=pltpu.VMEM), pl.BlockSpec(memory_space=pl.ANY)
    dma, v = pltpu.SemaphoreType.DMA, pltpu.VMEM
    result, new_state, new_conv = pl.pallas_call(
        kernel,
        name="layer",
        out_shape=(v(tokens.shape, BF16), v(rec_state.shape, F32), v((3, seqs, W), BF16)),
        in_specs=[hbm] * 18,
        out_specs=(vmem, vmem, vmem),
        scratch_shapes=[
            v(tokens.shape, BF16), v((D // W, W), BF16), v((TOK, seqs), I32), v((TOK, TOK), F32),
            v((seqs, W), F32), v((3, seqs, W), BF16), v((NT, W), F32), v((NT, W), BF16), v((D // W, W), BF16), v((TOK, W), BF16),
            v((D, 2 * W), BF16), v((NC * W, CW), BF16), v((W, W), BF16), v((W, W), BF16),
            v((DA, 2 * FW), BF16), v((DB, 2 * FW), BF16), v((FW, DA), BF16), v((FW, DB), BF16),
            v((16, CW), F32), v((NT, 16, CW), BF16),
            v((2, NZ, 16, CW + TAIL), BF16), v((NZ, 16, CW + TAIL), BF16), v((NZ, 16, CW + TAIL), BF16),
            v((NZ, 16, CW + TAIL), BF16),
            v((NE, 8, CA), BF16), v((NE, 8, CA), BF16),
            v((NZ, 2, ROWS, DA), BF16), v((NZ, 2 * ROWS, 2 * FW), F32), v((NZ, 2, ROWS, DA), BF16), v((NZ, ROWS, DA), BF16),
            v((NZ, 2, HALF, DA), BF16), v((2, 4, HALF, DA), BF16), v((2, 4, HALF, DA), BF16),
            v((NE, 8, CA), BF16), v((NE, 8, CA), BF16), v((16, 4), F32),
            v((NZ, 16, CB + TAIL), BF16), v((NE, 16, DB), BF16), v((2, NE, 16, DB), BF16), v((NZ, 2, ROWS, DB), BF16),
            v((2, NZ, ROWS, DB), BF16), v((NZ, ROWS, DB), BF16), v((NE, 16, DB), BF16), v((NE, 16, DB), BF16),
            v((NZ, 16, CB), BF16), v((NZ, 16, CB), BF16),
            dma((22,)), dma, dma((NT,)), dma, dma, dma, dma, dma, dma,
            dma, dma((NZ * 2,)), dma, dma((NZ * 2,)), dma, dma((NZ,)), dma, dma((8,)), dma((8,)), dma, dma,
            dma, dma, dma, dma((NE,)), dma, dma, dma, dma, dma, dma, dma, dma,
        ],
        compiler_params=pltpu.CompilerParams(
            collective_id=0, has_side_effects=True, vmem_limit_bytes=60 * 1024 * 1024
        ),
    )(
        tokens, first_gain.reshape(D // W, W), route_ids.T, route_weights, rec_state, conv_state.transpose(1, 0, 2),
        decay_logit.reshape(NT, W), rec_gain.reshape(NT, W), second_gain.reshape(D // W, W), conv_taps,
        proj_input, proj_gate, block_decay, block_input, proj_out, expert_gate, expert_up, expert_down,
    )
    return result, new_state, new_conv.transpose(1, 0, 2)


def solution(mesh):
    in_specs = (
        P(("ep", "tp"), None),
        P("ep", "tp"),
        P("ep", None, "tp"),
        P("ep", None),
        P(("ep", "tp"), None),
        P(),
        P(None, "tp"),
        P(None, "tp"),
        P(),
        P(),
        P(),
        P(),
        P(),
        P("tp", None),
        P(),
        P("ep", None, "tp"),
        P("ep", None, "tp"),
        P("ep", "tp", None),
    )
    out_specs = (P(("ep", "tp"), None), P("ep", "tp"), P("ep", None, "tp"))
    return jax.shard_map(
        per_device, mesh=mesh, in_specs=in_specs, out_specs=out_specs, check_vma=False
    )
```

```python
import jax
import jax.numpy as jnp
from jax import lax
from jax.experimental import pallas as pl
from jax.experimental.pallas import tpu as pltpu
from jax.sharding import PartitionSpec as P

MESH = pl.DeviceIdType.MESH
BF16, F32, I32 = jnp.bfloat16, jnp.float32, jnp.int32

EPS = 1e-06
CLAMP = 7.0
ALPHA = 1.702
RATE = 8.0

D = 4096
NC = 4
CW = D // NC
TOK = 4
NE = 16
NT = 16
NZ = 8
D_REC = 2048
W = 128
FW = 256
SLOTS = 2
ROWS = NE * SLOTS
HALF = ROWS // 2
QUARTER = ROWS // 4
TAIL = 128
EARLY = 5
CBI, CBO = 512, 384
CAI, CAO = CW - CBI, CW - CBO
DAI, DBI, DAO, DBO = NC * CAI, NC * CBI, NC * CAO, NC * CBO


def iota(shape, dim):
    return lax.broadcasted_iota(I32, shape, dim)


def onehot(cond):
    return jnp.where(cond, 1.0, 0.0).astype(F32)


def dot(a, b):
    return jnp.dot(a, b, preferred_element_type=F32)


def per_token(values):
    part = jnp.broadcast_to(jnp.sum(values, axis=1, keepdims=True), (NC * TOK, 128))
    total = part
    for c in range(1, NC):
        total = total + pltpu.roll(part, c * TOK, 0)
    return total[:, 0:1]


def spread(ref):
    values, shape = ref[...].astype(F32), (NC * TOK, 128)
    c_of = iota(shape, 0) // TOK
    blocks = []
    for i in range(CW // 128):
        block = jnp.broadcast_to(values[i : i + 1, :], shape)
        for c in range(1, NC):
            row = c * (CW // 128) + i
            block = jnp.where(c_of == c, jnp.broadcast_to(values[row : row + 1, :], shape), block)
        blocks.append(block)
    return jnp.concatenate(blocks, axis=1)


def minus_expm1(x):
    small = jnp.full_like(x, 1.0)
    for k in range(8, 1, -1):
        small = 1.0 + small * x * (1.0 / k)
    return jnp.where(x > -0.3, -x * small, 1.0 - jnp.exp(x))


def kernel(
    tokens_hbm, gain1_hbm, ids_hbm, weights_hbm, rec_hbm, conv_hbm, logit_hbm, rgain_hbm, gain2_hbm, taps_hbm,
    pin_hbm, pgate_hbm, bdec_hbm, binp_hbm, pout_hbm, eg_hbm, eu_hbm, ed_hbm,
    result_ref, state_ref, newconv_ref,
    tokens_ref, gain1_ref, ids_ref, weights_ref, rec_ref, conv_ref, logit_ref, rgain_ref, gain2_ref, taps_ref,
    wcat, w4, gates, wgu_a, wgu_b, wdown_a, wdown_b,
    tok_s, g1, pb, rp, sb, rb, ob, ib, xa, acc, part_a, rpart_a, sums, rright, rleft, ob2, ib2, rw_s,
    perm_s, expand_s, by_z_s, by_a_s, chosen_s,
    sg, tb, xr, xb, part_b, rpart_b, tb2, rr, cb, rcb,
    lsem, s1, r1, s2p, r2p, s2, r2, s3, r3, s4, r4, s4d, r4d, s5p, r5p, s5, r5r, r5l, s6, r6,
    sb1, rb1, sb2, rb2, sb2d, rb2d, sbp, rbp, sb3, rb3, sb4, rb4,
):
    ep = lax.axis_index("ep")
    tp = lax.axis_index("tp")
    z = tp // 2
    core = tp % 2
    other = 1 - core
    mate = (ep, z * 2 + other)
    y, x = ep // 4, ep % 4

    def remote(src, dst, ss, rs, dev):
        return pltpu.make_async_remote_copy(
            src_ref=src, dst_ref=dst, send_sem=ss, recv_sem=rs, device_id=dev, device_id_type=MESH
        )

    def all_of(ref, sem):
        pltpu.make_async_copy(ref, ref, sem).wait()

    def over(dy, dx):
        return ((y + dy + 4) % 4) * 4 + (x + dx + 4) % 4

    def along(d):
        return (z + d + NZ) % NZ

    def at_z(zz):
        return (ep, zz * 2 + core)

    barrier = pltpu.get_barrier_semaphore()
    pl.semaphore_signal(barrier, inc=1, device_id=mate, device_id_type=MESH)
    for d in range(1, NZ):
        pl.semaphore_signal(barrier, inc=1, device_id=at_z(along(d)), device_id_type=MESH)
    for d in range(1, NE):
        pl.semaphore_signal(barrier, inc=1, device_id=((ep + d) % NE, tp), device_id_type=MESH)

    smalls = [
        pltpu.make_async_copy(src, dst, lsem.at[7 + i])
        for i, (src, dst) in enumerate((
            (tokens_hbm, tokens_ref), (gain1_hbm, gain1_ref), (ids_hbm, ids_ref), (weights_hbm, weights_ref),
            (rec_hbm, rec_ref), (conv_hbm, conv_ref), (logit_hbm, logit_ref), (rgain_hbm, rgain_ref),
            (gain2_hbm, gain2_ref), (taps_hbm.at[:, pl.ds(pl.multiple_of(tp * W, W), W)], taps_ref),
        ))
    ]
    for load in smalls:
        load.start()
    loads = [
        pltpu.make_async_copy(pin_hbm, wcat.at[:, pl.ds(0, W)], lsem.at[0]),
        pltpu.make_async_copy(pgate_hbm, wcat.at[:, pl.ds(W, W)], lsem.at[0]),
        pltpu.make_async_copy(bdec_hbm.at[tp], gates.at[0], lsem.at[1]),
        pltpu.make_async_copy(binp_hbm.at[tp], gates.at[1], lsem.at[1]),
    ]
    for c in range(NC):
        loads.append(
            pltpu.make_async_copy(
                pout_hbm.at[:, pl.ds(c * CW, CW)], w4.at[pl.ds(c * W, W), :], lsem.at[2]
            )
        )
    for load in loads:
        load.start()
    for c in range(NC):
        for i, (hbm, col) in enumerate(((eg_hbm, 0), (eu_hbm, FW))):
            for dst, first, size, sem in ((wgu_a, 0, CAI, 3), (wgu_b, CAI, CBI, 4)):
                pltpu.make_async_copy(
                    hbm.at[0, pl.ds(c * CW + first, size), :],
                    dst.at[pl.ds(c * size, size), pl.ds(col, FW)],
                    lsem.at[sem],
                ).start()
        for dst, first, size, sem in ((wdown_a, 0, CAO, 5), (wdown_b, CAO, CBO, 6)):
            pltpu.make_async_copy(
                ed_hbm.at[0, :, pl.ds(c * CW + first, size)], dst.at[:, pl.ds(c * size, size)], lsem.at[sem]
            ).start()

    smalls[0].wait()
    smalls[1].wait()
    own = tokens_ref[...].astype(F32)
    for c in range(NC):
        tok_s[c * TOK : (c + 1) * TOK, :] = own[:, c * CW : (c + 1) * CW]
    values = tok_s[...]
    scale = lax.rsqrt(per_token(values * values) * (1.0 / D) + EPS)
    g1[tp] = (values * scale * spread(gain1_ref)).astype(BF16)

    pl.semaphore_wait(barrier, NZ + NE - 1)

    for d in (4, 3, 5, 2, 6, 1, 7):
        remote(g1.at[tp], g1.at[tp], s1, r1.at[z], at_z(along(d))).start()
    remote(g1.at[tp], g1.at[tp], s1, r1.at[NZ], mate).start()

    q4, r4e = (NC * TOK, W), 8
    row_n, row_c = iota(q4, 0) % TOK, iota(q4, 0) // TOK
    lane_e, lane_c, lane_s = iota(q4, 1) // r4e, (iota(q4, 1) // SLOTS) % NC, iota(q4, 1) % SLOTS
    pick_own = onehot(iota((NC * TOK, NE * TOK), 1) == tp * TOK + iota((NC * TOK, NE * TOK), 0) % TOK)
    smalls[2].wait()
    smalls[3].wait()
    all_ids = ids_ref[...].astype(F32).astype(BF16)
    own_ids = lax.dot_general(pick_own.astype(BF16), all_ids, (((1,), (1,)), ((), ())), preferred_element_type=F32)
    for c in range(NC):
        rw_s[c * TOK : (c + 1) * TOK, :] = weights_ref[...]
    hit = jnp.zeros(q4, F32)
    weighed = jnp.zeros(q4, F32)
    lane_ef = lane_e.astype(F32)
    for k in range(4):
        same = onehot(own_ids[:, k : k + 1] == lane_ef)
        hit = hit + same
        weighed = weighed + same * rw_s[:, k : k + 1]
    sq = (NC * TOK, NC * TOK)
    earlier = onehot(
        (iota(sq, 0) // TOK == iota(sq, 1) // TOK) & (iota(sq, 1) % TOK < iota(sq, 0) % TOK)
    )
    before = dot(earlier.astype(BF16), hit.astype(BF16))
    chosen = hit * onehot((before == lane_s.astype(F32)) & (row_c == lane_c))
    combine = chosen * weighed

    qn, rn = NZ * NC * TOK, NE * NZ * SLOTS
    big_q = (qn, rn)
    pick_core = onehot(
        iota((qn, NE * TOK), 1) == ((iota((qn, NE * TOK), 0) // 16) * 2 + core) * TOK + iota((qn, NE * TOK), 0) % TOK
    )
    core_ids = lax.dot_general(pick_core.astype(BF16), all_ids, (((1,), (1,)), ((), ())), preferred_element_type=F32)
    big_e = (iota(big_q, 1) // (NZ * SLOTS)).astype(F32)
    big_s = (iota(big_q, 1) % SLOTS).astype(F32)
    same_z = iota(big_q, 0) // 16 == (iota(big_q, 1) // SLOTS) % NZ
    big_hit = jnp.zeros(big_q, F32)
    for k in range(4):
        big_hit = big_hit + onehot(core_ids[:, k : k + 1] == big_e)
    qq = (qn, qn)
    big_earlier = onehot(
        (iota(qq, 0) // TOK == iota(qq, 1) // TOK) & (iota(qq, 1) % TOK < iota(qq, 0) % TOK)
    )
    big_before = dot(big_earlier.astype(BF16), big_hit.astype(BF16))
    big_chosen = big_hit * onehot((big_before == big_s) & same_z)
    c_of_q = (iota(big_q, 0) // TOK) % NC
    for c in range(NC):
        chosen_s[c] = jnp.where(c_of_q == c, big_chosen, 0.0).astype(BF16)

    big = NT * NC * TOK
    pr, pc = iota((big, big), 0), iota((big, big), 1)
    perm_s[...] = onehot(pc == ((pr // TOK) % NT) * 16 + (pr // 64) * TOK + pr % TOK).astype(BF16)
    er, et = iota((big, NT * TOK), 0), iota((big, NT * TOK), 1)
    expand_s[...] = onehot(et == (((er // 16) % NZ) * 2 + er // 128) * TOK + er % TOK).astype(BF16)
    tr, tc = iota((rn, rn), 0), iota((rn, rn), 1)
    by_z_s[...] = onehot(tc == ((tr // SLOTS) % NE) * 16 + (tr // ROWS) * SLOTS + tr % SLOTS).astype(BF16)
    by_a_s[...] = onehot(tr == ((tc // SLOTS) % NE) * 16 + (tc // ROWS) * SLOTS + tc % SLOTS).astype(BF16)

    for d in (1, 7, 2, 6, 3, 5, 4):
        zz = along(d)
        block = g1.at[zz * 2 + core]
        remote(block, block, s1, r1.at[zz], mate).wait_recv()
        remote(block, block, s1, r1.at[NZ], mate).start()
    all_of(g1.at[pl.ds(0, NZ)], r1.at[NZ])

    stacked = dot(perm_s[...], g1[...].reshape(big, CW)).astype(BF16)
    for load in smalls[4:]:
        load.wait()
    all_of(wcat, lsem.at[0])
    all_of(gates, lsem.at[1])
    both = jnp.zeros((NT * TOK, 2 * W), F32)
    for c in range(NC):
        both = both + dot(stacked[c * 64 : (c + 1) * 64, :], wcat[c * CW : (c + 1) * CW, :])
    joined = both.astype(BF16)
    branch_in, branch_gate = joined[:, :W].astype(F32), joined[:, W:].astype(F32)

    taps = taps_ref[...].astype(F32)
    conv = taps[3:4, :] * branch_in
    for tap in range(3):
        conv = conv + taps[tap : tap + 1, :] * conv_ref[tap].astype(F32)
    newconv_ref[0:2] = conv_ref[1:3]
    newconv_ref[2] = joined[:, :W]

    low = conv.astype(BF16)
    decay_gate = jax.nn.sigmoid(dot(low, gates[0]))
    input_gate = jax.nn.sigmoid(dot(low, gates[1]))
    mine = iota((NT, W), 0) == tp
    logit = jnp.sum(jnp.where(mine, logit_ref[...], 0.0), axis=0, keepdims=True)
    rgain = jnp.sum(jnp.where(mine, rgain_ref[...].astype(F32), 0.0), axis=0, keepdims=True)
    soft = jnp.maximum(-logit, 0.0) + jnp.log1p(jnp.exp(-jnp.abs(logit)))
    log_keep = -RATE * decay_gate * soft
    new_state = jnp.exp(log_keep) * rec_ref[...] + jnp.sqrt(minus_expm1(2.0 * log_keep)) * input_gate * conv
    state_ref[...] = new_state
    hidden = new_state * jax.nn.gelu(branch_gate)
    squares = jnp.broadcast_to(jnp.sum(hidden * hidden, axis=1, keepdims=True), (NT * TOK, W))

    wide = dot(expand_s[...], jnp.concatenate([(hidden * rgain).astype(BF16), squares.astype(BF16)], axis=1))
    gained, sq_wide = wide[:, :W], wide[:, W:]
    c_of = (iota((big, W), 0) // TOK) % NC
    all_of(w4, lsem.at[2])
    lhs = jnp.concatenate([jnp.where(c_of == c, gained, 0.0) for c in range(NC)], axis=1).astype(BF16)
    pb[:, :, :, 0:CW] = dot(lhs, w4[...]).astype(BF16).reshape(2, NZ, 16, CW)
    pb[:, :, :, CW : CW + TAIL] = sq_wide.astype(BF16).reshape(2, NZ, 16, TAIL)

    pair2 = pltpu.make_async_remote_copy(
        src_ref=pb.at[other], dst_ref=rp, send_sem=s2p, recv_sem=r2p, device_id=mate, device_id_type=MESH
    )
    pair2.start()
    pair2.wait_recv()

    def copy2(dev, slot):
        return pltpu.make_async_remote_copy(
            src_ref=sb.at[slot], dst_ref=rb.at[z], send_sem=s2, recv_sem=r2, device_id=dev, device_id_type=MESH
        )

    for d in (4, 3, 5, 2, 6, 1, 7):
        zz = along(d)
        sb[zz] = (pb[core, zz].astype(F32) + rp[zz].astype(F32)).astype(BF16)
        copy2(at_z(zz), zz).start()
    rb[z] = (pb[core, z].astype(F32) + rp[z].astype(F32)).astype(BF16)
    pltpu.make_async_copy(sb.at[pl.ds(0, NZ - 1)], rb.at[pl.ds(0, NZ - 1)], r2).wait()
    summed = jnp.zeros((16, CW + TAIL), F32)
    for zz in range(NZ):
        summed = summed + rb[zz].astype(F32)
    residual = tok_s[...] + summed[:, :CW] * lax.rsqrt(summed[:, CW : CW + 1] * (1.0 / D_REC) + EPS)
    scale = lax.rsqrt(per_token(residual * residual) * (1.0 / D) + EPS)
    second = (residual * scale * spread(gain2_ref)).astype(BF16)
    tok_s[...] = residual

    w_high = rw_s[...].astype(BF16).astype(F32)
    w_rest = rw_s[...] - w_high
    lane = iota((NC * TOK, TAIL), 1)
    tail = jnp.zeros((NC * TOK, TAIL), F32)
    for k in range(4):
        tail = jnp.where(lane == k, w_high[:, k : k + 1], tail)
        tail = jnp.where(lane == 4 + k, w_rest[:, k : k + 1], tail)
    sg[z, :, 0:CBI] = second[:, CAI:]
    sg[z, :, CBI:] = tail.astype(BF16)
    sent = lax.dot_general(
        chosen.astype(BF16), second[:, :CAI], (((0,), (0,)), ((), ())), preferred_element_type=F32
    )
    ob[...] = sent.reshape(NE, 8, CAI).astype(BF16)
    ib[ep] = ob[ep]
    for d in (4, 3, 5, 2, 6, 1, 7):
        remote(sg.at[z], sg.at[z], sb1, rb1, at_z(along(d))).start()

    ways = (
        (2, 2), (2, 1), (1, 3), (3, 2), (0, 2), (2, 3), (1, 2), (2, 0),
        (3, 1), (3, 3), (1, 1), (0, 3), (1, 0), (0, 1), (3, 0),
    )

    def to_experts(src, dst, ss, rs):
        for dy, dx in ways:
            e = over(dy, dx)
            remote(src.at[e], dst.at[ep], ss, rs, (e, tp)).start()

    to_experts(ob, ib, s3, r3)

    all_of(ib.at[pl.ds(0, NE - 1)], r3)
    own_rows = NE * 8
    sr, sc = iota((own_rows, own_rows), 0), iota((own_rows, own_rows), 1)
    turn = onehot(sc == ((sr // SLOTS) % NE) * 8 + (sr // ROWS) * SLOTS + sr % SLOTS).astype(BF16)
    turned = dot(turn, ib[...].astype(F32).reshape(own_rows, CAI).astype(BF16)).astype(BF16)
    for c in range(NC):
        xa[z, core, :, c * CAI : (c + 1) * CAI] = turned[c * ROWS : (c + 1) * ROWS, :]

    def copy4(zz, h, dev):
        block = xa.at[zz, core, pl.ds(h * HALF, HALF), :]
        return remote(block, block, s4, r4.at[zz * 2 + h], dev)

    def cross4(zz, h, side):
        block = xa.at[zz, side, pl.ds(h * HALF, HALF), :]
        return remote(block, block, s4d, r4d.at[zz], mate)

    right, left = at_z(along(1)), at_z(along(-1))
    for h in range(2):
        copy4(z, h, right).start()
        copy4(z, 1 - h, left).start()
    cross4(z, 0, core).start()
    cross4(z, 1, core).start()

    all_of(sg.at[pl.ds(0, NZ - 1)], rb1)
    group = sg[...].reshape(qn, CBI + TAIL)
    for c in range(NC):
        picked = lax.dot_general(
            chosen_s[c], group[:, :CBI], (((0,), (0,)), ((), ())), preferred_element_type=F32
        )
        tb[:, :, c * CBI : (c + 1) * CBI] = picked.reshape(NE, NZ * SLOTS, CBI).astype(BF16)
    for i, (dy, dx) in enumerate(ways):
        e = over(dy, dx)
        remote(tb.at[e], xr.at[core, ep], sb2, rb2.at[min(i // EARLY, 2)], (e, tp)).start()
    xr[core, ep] = tb[ep]
    remote(tb.at[ep], xr.at[core, ep], sb2d, rb2d, mate).start()

    def across(first, last, group):
        all_of(tb.at[pl.ds(0, last - first)], rb2.at[group])
        for dy, dx in ways[first:last]:
            source = over(-dy, -dx)
            block = xr.at[core, source]
            remote(block, block, sb2d, rb2d, mate).start()

    all_of(wgu_a, lsem.at[3])

    def first_part(*blocks):
        for zz in blocks:
            all_of(xa.at[zz, other], r4d.at[zz])
        rows = jnp.concatenate([xa[zz].reshape(2 * ROWS, DAI) for zz in blocks], axis=0)
        out = dot(rows, wgu_a[...])
        for i, zz in enumerate(blocks):
            acc[zz] = out[i * 2 * ROWS : (i + 1) * 2 * ROWS].reshape(2, ROWS, 2 * FW)

    def arrivals(s):
        for i in range(2):
            for h, way, hops, nxt in ((i, -1, 4 - i, right), (1 - i, 1, 4 - i, left)):
                if s <= hops:
                    zz = along(way * s)
                    copy4(zz, h, nxt).wait_recv()
                    if s < hops:
                        copy4(zz, h, nxt).start()
                    cross4(zz, h, core).start()

    def turn_over(side):
        xb[:, side] = dot(by_z_s[...], xr[side].reshape(rn, DBI)).astype(BF16).reshape(NZ, ROWS, DBI)

    arrivals(1)
    first_part(z)
    arrivals(2)
    first_part(along(1), along(-1))
    across(0, EARLY, 0)
    arrivals(3)
    across(EARLY, 2 * EARLY, 1)
    first_part(along(2), along(-2))
    across(2 * EARLY, len(ways), 2)
    arrivals(4)
    turn_over(core)
    all_of(wgu_b, lsem.at[4])
    all_of(wdown_a, lsem.at[5])
    all_of(wdown_b, lsem.at[6])
    first_part(along(3), along(-3), along(4))
    all_of(xr.at[core], rb2d)
    turn_over(other)

    def pair_a(zz):
        return remote(part_a.at[zz, other], rpart_a.at[zz], s5p, r5p.at[zz], mate)

    def finish(*blocks):
        rows = jnp.concatenate([xb[zz].reshape(2 * ROWS, DBI) for zz in blocks], axis=0)
        gu = jnp.concatenate([acc[zz].reshape(2 * ROWS, 2 * FW) for zz in blocks], axis=0) + dot(rows, wgu_b[...])
        gate, up = jnp.minimum(gu[:, :FW], CLAMP), jnp.clip(gu[:, FW:], -CLAMP, CLAMP)
        act = ((up + 1.0) * (gate * jax.nn.sigmoid(ALPHA * gate))).astype(BF16)
        out = dot(act, wdown_a[...]).astype(BF16)
        for i, zz in enumerate(blocks):
            part_a[zz] = out[2 * i * ROWS : 2 * (i + 1) * ROWS].reshape(2, ROWS, DAO)
            pair_a(zz).start()
        out = dot(act, wdown_b[...]).astype(BF16)
        for i, zz in enumerate(blocks):
            for side in range(2):
                at = (2 * i + side) * ROWS
                part_b[side, zz] = out[at : at + ROWS]
            remote(part_b.at[other, zz], rpart_b.at[zz], sbp, rbp, mate).start()

    def pair_sum(zz, h):
        rows = slice(h * QUARTER, (h + 1) * QUARTER)
        return part_a[zz, core, rows, :].astype(F32) + rpart_a[zz, rows, :].astype(F32)

    def copy5(zz, h, hop, to_right):
        return remote(
            sums.at[zz, h],
            (rright if to_right else rleft).at[h, hop],
            s5,
            (r5r if to_right else r5l).at[h * 4 + hop],
            right if to_right else left,
        )

    def got5(h, hop, from_left):
        return (rright if from_left else rleft)[h, hop].astype(F32)

    def pass_on(hop, h, to_right):
        zz = along(hop if to_right else -hop)
        total = pair_sum(zz, h)
        if hop < (4 - h // 2 if to_right else 3 + h // 2):
            copy5(zz, h, hop, to_right).wait_recv()
            total = total + got5(h, hop, to_right)
        sums[zz, h] = total.astype(BF16)
        copy5(zz, h, hop - 1, to_right).start()

    def pair_sum(zz, h):
        rows = slice(h * QUARTER, (h + 1) * QUARTER)
        return part_a[zz, core, rows, :].astype(F32) + rpart_a[zz, rows, :].astype(F32)

    def copy5(zz, h, hop, to_right):
        return remote(
            sums.at[zz, h],
            (rright if to_right else rleft).at[h, hop],
            s5,
            (r5r if to_right else r5l).at[h * 4 + hop],
            right if to_right else left,
        )

    def got5(h, hop, from_left):
        return (rright if from_left else rleft)[h, hop].astype(F32)

    def pass_on(hop, h, to_right):
        zz = along(hop if to_right else -hop)
        total = pair_sum(zz, h)
        if hop < (4 - h // 2 if to_right else 3 + h // 2):
            copy5(zz, h, hop, to_right).wait_recv()
            total = total + got5(h, hop, to_right)
        sums[zz, h] = total.astype(BF16)
        copy5(zz, h, hop - 1, to_right).start()

    def shorter(hop):
        for h in (0, 1):
            pass_on(hop, h + 2, True)
            pass_on(hop, h, False)

    def longer(hop):
        for h in (0, 1):
            pass_on(hop, h, True)
            pass_on(hop, h + 2, False)

    finish(along(3), along(-3))
    finish(along(4), z)
    pair_a(along(3)).wait_recv()
    pair_a(along(-3)).wait_recv()
    shorter(3)
    finish(along(2), along(-2))
    pair_a(along(4)).wait_recv()
    longer(4)
    finish(along(1), along(-1))
    pair_a(along(2)).wait_recv()
    pair_a(along(-2)).wait_recv()
    shorter(2)

    half_sum = dot(by_a_s[...], part_b[core].reshape(rn, DBO))
    all_of(rpart_b, rbp)
    half_sum = half_sum + dot(by_a_s[...], rpart_b[...].reshape(rn, DBO))
    tb2[...] = half_sum.astype(BF16).reshape(NE, NZ * SLOTS, DBO)
    to_experts(tb2, rr, sb3, rb3)
    rr[ep] = tb2[ep]

    longer(3)
    pair_a(along(1)).wait_recv()
    pair_a(along(-1)).wait_recv()
    shorter(1)
    longer(2)
    longer(1)
    pair_a(z).wait_recv()
    for h in (2, 3, 0, 1):
        total = pair_sum(z, h)
        for to_right in (True, False):
            copy5(z, h, 0, to_right).wait_recv()
            total = total + got5(h, 0, to_right)
        sums[z, h] = total.astype(BF16)

    final = sums[z].astype(F32).reshape(ROWS, DAO).astype(BF16)
    mine = jnp.concatenate([final[:, c * CAO : (c + 1) * CAO] for c in range(NC)], axis=0)
    back = onehot(sr == ((sc // SLOTS) % NE) * 8 + (sc // ROWS) * SLOTS + sc % SLOTS).astype(BF16)
    ob2[...] = dot(back, mine).reshape(NE, 8, CAO).astype(BF16)
    ib2[ep] = ob2[ep]
    to_experts(ob2, ib2, s6, r6)

    def in_two(values):
        high = values.astype(BF16)
        return high, (values - high.astype(F32)).astype(BF16)

    tails = sg[...].reshape(qn, CBI + TAIL)[:, CBI:].astype(F32)
    big_weighed = jnp.zeros(big_q, F32)
    for k in range(4):
        weight = tails[:, k : k + 1] + tails[:, 4 + k : 5 + k]
        big_weighed = big_weighed + onehot(core_ids[:, k : k + 1] == big_e) * weight
    big_high, big_low = in_two(big_chosen * big_weighed)
    all_of(rr.at[pl.ds(0, NE - 1)], rb3)
    taken = rr[...].reshape(rn, DBO)
    mixed = jnp.zeros((qn, CBO), F32)
    for c in range(NC):
        piece = taken[:, c * CBO : (c + 1) * CBO]
        for factor in (big_low, big_high):
            mixed = mixed + dot(jnp.where(c_of_q == c, factor.astype(F32), 0.0).astype(BF16), piece)
    cb[...] = mixed.astype(BF16).reshape(NZ, 16, CBO)
    for d in (4, 3, 5, 2, 6, 1, 7):
        remote(cb.at[along(d)], rcb.at[z], sb4, rb4, at_z(along(d))).start()
    rcb[z] = cb[z]

    high = combine.astype(BF16)
    rest = combine - high.astype(F32)
    middle, lowest = in_two(rest)
    all_of(ib2.at[pl.ds(0, NE - 1)], r6)
    returned = ib2[...].astype(F32).reshape(NE * 8, CAO).astype(BF16)
    mix_a = dot(lowest, returned) + dot(middle, returned) + dot(high, returned)
    all_of(rcb.at[pl.ds(0, NZ - 1)], rb4)
    mix_b = jnp.zeros((16, CBO), F32)
    for zz in range(NZ):
        mix_b = mix_b + rcb[zz].astype(F32)
    tok_s[:, :CAO] = tok_s[:, :CAO] + mix_a
    tok_s[:, CAO:] = tok_s[:, CAO:] + mix_b
    for c in range(NC):
        result_ref[:, c * CW : (c + 1) * CW] = tok_s[c * TOK : (c + 1) * TOK, :].astype(BF16)

    all_of(g1.at[pl.ds(0, NT - 1)], s1)
    pair2.wait_send()
    all_of(sb.at[pl.ds(0, NZ - 1)], s2)
    all_of(ob.at[pl.ds(0, NE - 1)], s3)
    all_of(xa.at[pl.ds(0, NZ - 1), 0], s4)
    all_of(xa.at[:, 0], s4d)
    all_of(rpart_a, s5p)
    all_of(sums.at[pl.ds(0, NZ - 1)], s5)
    all_of(ob2.at[pl.ds(0, NE - 1)], s6)
    all_of(sg.at[pl.ds(0, NZ - 1)], sb1)
    all_of(tb.at[pl.ds(0, NE - 1)], sb2)
    all_of(tb, sb2d)
    all_of(rpart_b, sbp)
    all_of(tb2.at[pl.ds(0, NE - 1)], sb3)
    all_of(cb.at[pl.ds(0, NZ - 1)], sb4)


def per_device(
    tokens, rec_state, conv_state, route_ids, route_weights, first_gain, proj_input, proj_gate, conv_taps,
    decay_logit, block_decay, block_input, rec_gain, proj_out, second_gain, expert_gate, expert_up, expert_down,
):
    seqs = rec_state.shape[0]
    vmem, hbm = pl.BlockSpec(memory_space=pltpu.VMEM), pl.BlockSpec(memory_space=pl.ANY)
    dma, v = pltpu.SemaphoreType.DMA, pltpu.VMEM
    result, new_state, new_conv = pl.pallas_call(
        kernel,
        name="layer",
        out_shape=(v(tokens.shape, BF16), v(rec_state.shape, F32), v((3, seqs, W), BF16)),
        in_specs=[hbm] * 18,
        out_specs=(vmem, vmem, vmem),
        scratch_shapes=[
            v(tokens.shape, BF16), v((D // W, W), BF16), v((TOK, seqs), I32), v((TOK, TOK), F32),
            v((seqs, W), F32), v((3, seqs, W), BF16), v((NT, W), F32), v((NT, W), BF16), v((D // W, W), BF16), v((TOK, W), BF16),
            v((D, 2 * W), BF16), v((NC * W, CW), BF16), v((2, W, W), BF16),
            v((DAI, 2 * FW), BF16), v((DBI, 2 * FW), BF16), v((FW, DAO), BF16), v((FW, DBO), BF16),
            v((16, CW), F32), v((NT, 16, CW), BF16),
            v((2, NZ, 16, CW + TAIL), BF16), v((NZ, 16, CW + TAIL), BF16), v((NZ, 16, CW + TAIL), BF16),
            v((NZ, 16, CW + TAIL), BF16),
            v((NE, 8, CAI), BF16), v((NE, 8, CAI), BF16),
            v((NZ, 2, ROWS, DAI), BF16), v((NZ, 2, ROWS, 2 * FW), F32), v((NZ, 2, ROWS, DAO), BF16), v((NZ, ROWS, DAO), BF16),
            v((NZ, 4, QUARTER, DAO), BF16), v((4, 4, QUARTER, DAO), BF16), v((4, 4, QUARTER, DAO), BF16),
            v((NE, 8, CAO), BF16), v((NE, 8, CAO), BF16), v((16, 4), F32),
            v((256, 256), BF16), v((256, 64), BF16), v((256, 256), BF16), v((256, 256), BF16), v((NC, 128, 256), BF16),
            v((NZ, 16, CBI + TAIL), BF16), v((NE, 16, DBI), BF16), v((2, NE, 16, DBI), BF16), v((NZ, 2, ROWS, DBI), BF16),
            v((2, NZ, ROWS, DBO), BF16), v((NZ, ROWS, DBO), BF16), v((NE, 16, DBO), BF16), v((NE, 16, DBO), BF16),
            v((NZ, 16, CBO), BF16), v((NZ, 16, CBO), BF16),
            dma((17,)), dma, dma((NZ + 1,)), dma, dma, dma, dma, dma, dma,
            dma, dma((NZ * 2,)), dma, dma((NZ,)), dma, dma((NZ,)), dma, dma((16,)), dma((16,)), dma, dma,
            dma, dma, dma, dma((3,)), dma, dma, dma, dma, dma, dma, dma, dma,
        ],
        compiler_params=pltpu.CompilerParams(
            collective_id=0, has_side_effects=True, vmem_limit_bytes=60 * 1024 * 1024
        ),
    )(
        tokens, first_gain.reshape(D // W, W), route_ids.T, route_weights, rec_state, conv_state.transpose(1, 0, 2),
        decay_logit.reshape(NT, W), rec_gain.reshape(NT, W), second_gain.reshape(D // W, W), conv_taps,
        proj_input, proj_gate, block_decay, block_input, proj_out, expert_gate, expert_up, expert_down,
    )
    def store(a_ref, b_ref, c_ref, a_hbm, b_hbm, c_hbm, sem):
        copies = [
            pltpu.make_async_copy(src, dst, sem.at[i])
            for i, (src, dst) in enumerate(((a_ref, a_hbm), (b_ref, b_hbm), (c_ref, c_hbm)))
        ]
        for copy in copies:
            copy.start()
        for copy in copies:
            copy.wait()

    outs = tuple(pltpu.with_memory_space_constraint(o, pltpu.VMEM) for o in (result, new_state, new_conv))
    result, new_state, new_conv = pl.pallas_call(
        store,
        name="store",
        out_shape=tuple(jax.ShapeDtypeStruct(o.shape, o.dtype) for o in outs),
        in_specs=[vmem] * 3,
        out_specs=(hbm,) * 3,
        scratch_shapes=[dma((3,))],
    )(*outs)
    return result, new_state, new_conv.transpose(1, 0, 2)


def solution(mesh):
    in_specs = (
        P(("ep", "tp"), None),
        P("ep", "tp"),
        P("ep", None, "tp"),
        P("ep", None),
        P(("ep", "tp"), None),
        P(),
        P(None, "tp"),
        P(None, "tp"),
        P(),
        P(),
        P(),
        P(),
        P(),
        P("tp", None),
        P(),
        P("ep", None, "tp"),
        P("ep", None, "tp"),
        P("ep", "tp", None),
    )
    out_specs = (P(("ep", "tp"), None), P("ep", "tp"), P("ep", None, "tp"))
    return jax.shard_map(
        per_device, mesh=mesh, in_specs=in_specs, out_specs=out_specs, check_vma=False
    )
```

```python
import jax
import jax.numpy as jnp
from jax import lax
from jax.experimental import pallas as pl
from jax.experimental.pallas import tpu as pltpu
from jax.sharding import PartitionSpec as P

MESH = pl.DeviceIdType.MESH
BF16, F32, I32 = jnp.bfloat16, jnp.float32, jnp.int32

EPS = 1e-06
CLAMP = 7.0
ALPHA = 1.702
RATE = 8.0

D = 4096
NC = 4
CW = D // NC
TOK = 4
NE = 16
NT = 16
NZ = 8
D_REC = 2048
W = 128
FW = 256
SLOTS = 2
ROWS = NE * SLOTS
HALF = ROWS // 2
QUARTER = ROWS // 4
TAIL = 128
EARLY = 5
CBI, CBO = 512, 384
CAI, CAO = CW - CBI, CW - CBO
DAI, DBI, DAO, DBO = NC * CAI, NC * CBI, NC * CAO, NC * CBO


def iota(shape, dim):
    return lax.broadcasted_iota(I32, shape, dim)


def onehot(cond):
    return jnp.where(cond, 1.0, 0.0).astype(F32)


def dot(a, b):
    return jnp.dot(a, b, preferred_element_type=F32)


def per_token(values):
    part = jnp.broadcast_to(jnp.sum(values, axis=1, keepdims=True), (NC * TOK, 128))
    total = part
    for c in range(1, NC):
        total = total + pltpu.roll(part, c * TOK, 0)
    return total[:, 0:1]


def spread(ref):
    values, shape = ref[...].astype(F32), (NC * TOK, 128)
    c_of = iota(shape, 0) // TOK
    blocks = []
    for i in range(CW // 128):
        block = jnp.broadcast_to(values[i : i + 1, :], shape)
        for c in range(1, NC):
            row = c * (CW // 128) + i
            block = jnp.where(c_of == c, jnp.broadcast_to(values[row : row + 1, :], shape), block)
        blocks.append(block)
    return jnp.concatenate(blocks, axis=1)


def minus_expm1(x):
    small = jnp.full_like(x, 1.0)
    for k in range(8, 1, -1):
        small = 1.0 + small * x * (1.0 / k)
    return jnp.where(x > -0.3, -x * small, 1.0 - jnp.exp(x))


def kernel(
    tokens_hbm, gain1_hbm, ids_hbm, weights_hbm, rec_hbm, conv_hbm, logit_hbm, rgain_hbm, gain2_hbm, taps_hbm,
    pin_hbm, pgate_hbm, bdec_hbm, binp_hbm, pout_hbm, eg_hbm, eu_hbm, ed_hbm,
    result_ref, state_ref, newconv_ref,
    tokens_ref, gain1_ref, ids_ref, weights_ref, rec_ref, conv_ref, logit_ref, rgain_ref, gain2_ref, taps_ref,
    wcat, w4, gates, wgu_a, wgu_b, wdown_a, wdown_b,
    tok_s, g1, pb, rp, sb, rb, sqs, sqr, ob, ib, xa, acc, part_a, rpart_a, sums, rright, rleft, ob2, ib2, rw_s,
    perm_s, expand_s, by_z_s, by_a_s, chosen_s,
    sg, tb, xr, acc_b, part_b, rpart_b, tb2, rr, cb, rcb,
    lsem, s1, s2q, r2q, r1, s2p, r2p, s2, r2, s3, r3, s4, r4, s4d, r4d, s5p, r5p, s5, r5r, r5l, s6, r6,
    sb1, rb1, sb2, rb2, sb2d, rb2d, sbp, rbp, sb3, rb3, sb4, rb4,
):
    ep = lax.axis_index("ep")
    tp = lax.axis_index("tp")
    z = tp // 2
    core = tp % 2
    other = 1 - core
    mate = (ep, z * 2 + other)
    y, x = ep // 4, ep % 4

    def remote(src, dst, ss, rs, dev):
        return pltpu.make_async_remote_copy(
            src_ref=src, dst_ref=dst, send_sem=ss, recv_sem=rs, device_id=dev, device_id_type=MESH
        )

    def all_of(ref, sem):
        pltpu.make_async_copy(ref, ref, sem).wait()

    def over(dy, dx):
        return ((y + dy + 4) % 4) * 4 + (x + dx + 4) % 4

    def along(d):
        return (z + d + NZ) % NZ

    def at_z(zz):
        return (ep, zz * 2 + core)

    barrier = pltpu.get_barrier_semaphore()
    pl.semaphore_signal(barrier, inc=1, device_id=mate, device_id_type=MESH)
    for d in range(1, NZ):
        pl.semaphore_signal(barrier, inc=1, device_id=at_z(along(d)), device_id_type=MESH)
    for d in range(1, NE):
        pl.semaphore_signal(barrier, inc=1, device_id=((ep + d) % NE, tp), device_id_type=MESH)

    smalls = [
        pltpu.make_async_copy(src, dst, lsem.at[7 + i])
        for i, (src, dst) in enumerate((
            (tokens_hbm, tokens_ref), (gain1_hbm, gain1_ref), (ids_hbm, ids_ref), (weights_hbm, weights_ref),
            (rec_hbm, rec_ref), (conv_hbm, conv_ref), (logit_hbm, logit_ref), (rgain_hbm, rgain_ref),
            (gain2_hbm, gain2_ref), (taps_hbm.at[:, pl.ds(pl.multiple_of(tp * W, W), W)], taps_ref),
        ))
    ]
    for load in smalls:
        load.start()
    loads = [
        pltpu.make_async_copy(pin_hbm, wcat.at[:, pl.ds(0, W)], lsem.at[0]),
        pltpu.make_async_copy(pgate_hbm, wcat.at[:, pl.ds(W, W)], lsem.at[0]),
        pltpu.make_async_copy(bdec_hbm.at[tp], gates.at[0], lsem.at[1]),
        pltpu.make_async_copy(binp_hbm.at[tp], gates.at[1], lsem.at[1]),
    ]
    for c in range(NC):
        loads.append(
            pltpu.make_async_copy(
                pout_hbm.at[:, pl.ds(c * CW, CW)], w4.at[pl.ds(c * W, W), :], lsem.at[2]
            )
        )
    for load in loads:
        load.start()
    for c in range(NC):
        for i, (hbm, col) in enumerate(((eg_hbm, 0), (eu_hbm, FW))):
            for dst, first, size, sem in ((wgu_a, 0, CAI, 3), (wgu_b, CAI, CBI, 4)):
                pltpu.make_async_copy(
                    hbm.at[0, pl.ds(c * CW + first, size), :],
                    dst.at[pl.ds(c * size, size), pl.ds(col, FW)],
                    lsem.at[sem],
                ).start()
        for dst, first, size, sem in ((wdown_a, 0, CAO, 5), (wdown_b, CAO, CBO, 6)):
            pltpu.make_async_copy(
                ed_hbm.at[0, :, pl.ds(c * CW + first, size)], dst.at[:, pl.ds(c * size, size)], lsem.at[sem]
            ).start()

    smalls[0].wait()
    smalls[1].wait()
    own = tokens_ref[...].astype(F32)
    for c in range(NC):
        tok_s[c * TOK : (c + 1) * TOK, :] = own[:, c * CW : (c + 1) * CW]
    values = tok_s[...]
    scale = lax.rsqrt(per_token(values * values) * (1.0 / D) + EPS)
    g1[tp] = (values * scale * spread(gain1_ref)).astype(BF16)

    pl.semaphore_wait(barrier, NZ + NE - 1)

    for d in (4, 3, 5, 2, 6, 1, 7):
        remote(g1.at[tp], g1.at[tp], s1, r1.at[z], at_z(along(d))).start()
    remote(g1.at[tp], g1.at[tp], s1, r1.at[NZ], mate).start()

    q4, r4e = (NC * TOK, W), 8
    row_n, row_c = iota(q4, 0) % TOK, iota(q4, 0) // TOK
    lane_e, lane_c, lane_s = iota(q4, 1) // r4e, (iota(q4, 1) // SLOTS) % NC, iota(q4, 1) % SLOTS
    pick_own = onehot(iota((NC * TOK, NE * TOK), 1) == tp * TOK + iota((NC * TOK, NE * TOK), 0) % TOK)
    smalls[2].wait()
    smalls[3].wait()
    all_ids = ids_ref[...].astype(F32).astype(BF16)
    own_ids = lax.dot_general(pick_own.astype(BF16), all_ids, (((1,), (1,)), ((), ())), preferred_element_type=F32)
    for c in range(NC):
        rw_s[c * TOK : (c + 1) * TOK, :] = weights_ref[...]
    hit = jnp.zeros(q4, F32)
    weighed = jnp.zeros(q4, F32)
    lane_ef = lane_e.astype(F32)
    for k in range(4):
        same = onehot(own_ids[:, k : k + 1] == lane_ef)
        hit = hit + same
        weighed = weighed + same * rw_s[:, k : k + 1]
    sq = (NC * TOK, NC * TOK)
    earlier = onehot(
        (iota(sq, 0) // TOK == iota(sq, 1) // TOK) & (iota(sq, 1) % TOK < iota(sq, 0) % TOK)
    )
    before = dot(earlier.astype(BF16), hit.astype(BF16))
    chosen = hit * onehot((before == lane_s.astype(F32)) & (row_c == lane_c))
    combine = chosen * weighed

    qn, rn = NZ * NC * TOK, NE * NZ * SLOTS
    big_q = (qn, rn)
    pick_core = onehot(
        iota((qn, NE * TOK), 1) == ((iota((qn, NE * TOK), 0) // 16) * 2 + core) * TOK + iota((qn, NE * TOK), 0) % TOK
    )
    core_ids = lax.dot_general(pick_core.astype(BF16), all_ids, (((1,), (1,)), ((), ())), preferred_element_type=F32)
    big_e = (iota(big_q, 1) // (NZ * SLOTS)).astype(F32)
    big_s = (iota(big_q, 1) % SLOTS).astype(F32)
    same_z = iota(big_q, 0) // 16 == (iota(big_q, 1) // SLOTS) % NZ
    big_hit = jnp.zeros(big_q, F32)
    for k in range(4):
        big_hit = big_hit + onehot(core_ids[:, k : k + 1] == big_e)
    qq = (qn, qn)
    big_earlier = onehot(
        (iota(qq, 0) // TOK == iota(qq, 1) // TOK) & (iota(qq, 1) % TOK < iota(qq, 0) % TOK)
    )
    big_before = dot(big_earlier.astype(BF16), big_hit.astype(BF16))
    big_chosen = big_hit * onehot((big_before == big_s) & same_z)
    c_of_q = (iota(big_q, 0) // TOK) % NC
    for c in range(NC):
        chosen_s[c] = jnp.where(c_of_q == c, big_chosen, 0.0).astype(BF16)

    big = NT * NC * TOK
    pr, pc = iota((big, big), 0), iota((big, big), 1)
    perm_s[...] = onehot(pc == ((pr // TOK) % NT) * 16 + (pr // 64) * TOK + pr % TOK).astype(BF16)
    er, et = iota((big, NT * TOK), 0), iota((big, NT * TOK), 1)
    expand_s[...] = onehot(et == (((er // 16) % NZ) * 2 + er // 128) * TOK + er % TOK).astype(BF16)
    tr, tc = iota((rn, rn), 0), iota((rn, rn), 1)
    by_z_s[...] = onehot(tc == ((tr // SLOTS) % NE) * 16 + (tr // ROWS) * SLOTS + tr % SLOTS).astype(BF16)
    by_a_s[...] = onehot(tr == ((tc // SLOTS) % NE) * 16 + (tc // ROWS) * SLOTS + tc % SLOTS).astype(BF16)

    for d in (1, 7, 2, 6, 3, 5, 4):
        zz = along(d)
        block = g1.at[zz * 2 + core]
        remote(block, block, s1, r1.at[zz], mate).wait_recv()
        remote(block, block, s1, r1.at[NZ], mate).start()
    all_of(g1.at[pl.ds(0, NZ)], r1.at[NZ])

    stacked = dot(perm_s[...], g1[...].reshape(big, CW)).astype(BF16)
    for load in smalls[4:]:
        load.wait()
    all_of(wcat, lsem.at[0])
    all_of(gates, lsem.at[1])
    both = jnp.zeros((NT * TOK, 2 * W), F32)
    for c in range(NC):
        both = both + dot(stacked[c * 64 : (c + 1) * 64, :], wcat[c * CW : (c + 1) * CW, :])
    joined = both.astype(BF16)
    branch_in, branch_gate = joined[:, :W].astype(F32), joined[:, W:].astype(F32)

    taps = taps_ref[...].astype(F32)
    conv = taps[3:4, :] * branch_in
    for tap in range(3):
        conv = conv + taps[tap : tap + 1, :] * conv_ref[tap].astype(F32)
    newconv_ref[0:2] = conv_ref[1:3]
    newconv_ref[2] = joined[:, :W]

    low = conv.astype(BF16)
    decay_gate = jax.nn.sigmoid(dot(low, gates[0]))
    input_gate = jax.nn.sigmoid(dot(low, gates[1]))
    mine = iota((NT, W), 0) == tp
    logit = jnp.sum(jnp.where(mine, logit_ref[...], 0.0), axis=0, keepdims=True)
    rgain = jnp.sum(jnp.where(mine, rgain_ref[...].astype(F32), 0.0), axis=0, keepdims=True)
    soft = jnp.maximum(-logit, 0.0) + jnp.log1p(jnp.exp(-jnp.abs(logit)))
    log_keep = -RATE * decay_gate * soft
    new_state = jnp.exp(log_keep) * rec_ref[...] + jnp.sqrt(minus_expm1(2.0 * log_keep)) * input_gate * conv
    state_ref[...] = new_state
    hidden = new_state * jax.nn.gelu(branch_gate)
    squares = jnp.broadcast_to(jnp.sum(hidden * hidden, axis=1, keepdims=True), (NT * TOK, W))

    wide = dot(expand_s[...], jnp.concatenate([(hidden * rgain).astype(BF16), squares.astype(BF16)], axis=1))
    gained, sq_wide = wide[:, :W], wide[:, W:]
    c_of = (iota((big, W), 0) // TOK) % NC
    all_of(w4, lsem.at[2])
    lhs = jnp.concatenate([jnp.where(c_of == c, gained, 0.0) for c in range(NC)], axis=1).astype(BF16)
    pb[:, :, :, 0:CW] = dot(lhs, w4[...]).astype(BF16).reshape(2, NZ, 16, CW)
    pb[:, :, :, CW : CW + TAIL] = sq_wide.astype(BF16).reshape(2, NZ, 16, TAIL)

    pair2 = pltpu.make_async_remote_copy(
        src_ref=pb.at[other], dst_ref=rp, send_sem=s2p, recv_sem=r2p, device_id=mate, device_id_type=MESH
    )
    pair2.start()
    pair2.wait_recv()

    row_of, lane_of = iota((NC * TOK, TAIL), 0), iota((NC * TOK, TAIL), 1)

    def in_a_row(zz):
        total = pb[core, zz, :, CW:].astype(F32) + rp[zz, :, CW:].astype(F32)
        return jnp.sum(jnp.where(row_of == lane_of, total, 0.0), axis=0, keepdims=True)

    for d in (4, 3, 5, 2, 6, 1, 7):
        zz = along(d)
        sb[zz] = (pb[core, zz, :, :CW].astype(F32) + rp[zz, :, :CW].astype(F32)).astype(BF16)
        sqs[zz] = in_a_row(zz)
        remote(sqs.at[zz], sqr.at[z], s2q, r2q, at_z(zz)).start()
        remote(sb.at[zz], rb.at[z], s2, r2, at_z(zz)).start()
    sqr[z] = in_a_row(z)
    rb[z] = (pb[core, z, :, :CW].astype(F32) + rp[z, :, :CW].astype(F32)).astype(BF16)
    all_of(sqr.at[pl.ds(0, NZ - 1)], r2q)
    own_row = sqr[0]
    for zz in range(1, NZ):
        own_row = own_row + sqr[zz]
    own_squares = jnp.sum(
        jnp.where(row_of == lane_of, jnp.broadcast_to(own_row, (NC * TOK, TAIL)), 0.0), axis=1, keepdims=True
    )
    all_of(rb.at[pl.ds(0, NZ - 1)], r2)
    summed = jnp.zeros((16, CW), F32)
    for zz in range(NZ):
        summed = summed + rb[zz].astype(F32)
    residual = tok_s[...] + summed * lax.rsqrt(own_squares * (1.0 / D_REC) + EPS)
    scale = lax.rsqrt(per_token(residual * residual) * (1.0 / D) + EPS)
    second = (residual * scale * spread(gain2_ref)).astype(BF16)
    tok_s[...] = residual

    w_high = rw_s[...].astype(BF16).astype(F32)
    w_rest = rw_s[...] - w_high
    lane = iota((NC * TOK, TAIL), 1)
    tail = jnp.zeros((NC * TOK, TAIL), F32)
    for k in range(4):
        tail = jnp.where(lane == k, w_high[:, k : k + 1], tail)
        tail = jnp.where(lane == 4 + k, w_rest[:, k : k + 1], tail)
    sg[z, :, 0:CBI] = second[:, CAI:]
    sg[z, :, CBI:] = tail.astype(BF16)
    sent = lax.dot_general(
        chosen.astype(BF16), second[:, :CAI], (((0,), (0,)), ((), ())), preferred_element_type=F32
    )
    ob[...] = sent.reshape(NE, 8, CAI).astype(BF16)
    ib[ep] = ob[ep]
    for d in (4, 3, 5, 2, 6, 1, 7):
        remote(sg.at[z], sg.at[z], sb1, rb1, at_z(along(d))).start()

    ways = (
        (2, 2), (2, 1), (1, 3), (3, 2), (0, 2), (2, 3), (1, 2), (2, 0),
        (3, 1), (3, 3), (1, 1), (0, 3), (1, 0), (0, 1), (3, 0),
    )

    def to_experts(src, dst, ss, rs):
        for dy, dx in ways:
            e = over(dy, dx)
            remote(src.at[e], dst.at[ep], ss, rs, (e, tp)).start()

    to_experts(ob, ib, s3, r3)

    all_of(ib.at[pl.ds(0, NE - 1)], r3)
    own_rows = NE * 8
    sr, sc = iota((own_rows, own_rows), 0), iota((own_rows, own_rows), 1)
    turn = onehot(sc == ((sr // SLOTS) % NE) * 8 + (sr // ROWS) * SLOTS + sr % SLOTS).astype(BF16)
    turned = dot(turn, ib[...].astype(F32).reshape(own_rows, CAI).astype(BF16)).astype(BF16)
    for c in range(NC):
        xa[z, core, :, c * CAI : (c + 1) * CAI] = turned[c * ROWS : (c + 1) * ROWS, :]

    def copy4(zz, h, dev):
        block = xa.at[zz, core, pl.ds(h * HALF, HALF), :]
        return remote(block, block, s4, r4.at[zz * 2 + h], dev)

    def cross4(zz, h, side):
        block = xa.at[zz, side, pl.ds(h * HALF, HALF), :]
        return remote(block, block, s4d, r4d.at[zz], mate)

    right, left = at_z(along(1)), at_z(along(-1))
    for h in range(2):
        copy4(z, h, right).start()
        copy4(z, 1 - h, left).start()
    cross4(z, 0, core).start()
    cross4(z, 1, core).start()

    all_of(sg.at[pl.ds(0, NZ - 1)], rb1)
    group = sg[...].reshape(qn, CBI + TAIL)
    for c in range(NC):
        picked = lax.dot_general(
            chosen_s[c], group[:, :CBI], (((0,), (0,)), ((), ())), preferred_element_type=F32
        )
        tb[:, :, c * CBI : (c + 1) * CBI] = picked.reshape(NE, NZ * SLOTS, CBI).astype(BF16)
    for i, (dy, dx) in enumerate(ways):
        e = over(dy, dx)
        remote(tb.at[e], xr.at[core, ep], sb2, rb2.at[min(i // EARLY, 2)], (e, tp)).start()
    xr[core, ep] = tb[ep]
    remote(tb.at[ep], xr.at[core, ep], sb2d, rb2d, mate).start()

    def across(first, last, group):
        all_of(tb.at[pl.ds(0, last - first)], rb2.at[group])
        for dy, dx in ways[first:last]:
            source = over(-dy, -dx)
            block = xr.at[core, source]
            remote(block, block, sb2d, rb2d, mate).start()

    all_of(wgu_a, lsem.at[3])

    def first_part(*blocks):
        for zz in blocks:
            all_of(xa.at[zz, other], r4d.at[zz])
        rows = jnp.concatenate([xa[zz].reshape(2 * ROWS, DAI) for zz in blocks], axis=0)
        out = dot(rows, wgu_a[...])
        for i, zz in enumerate(blocks):
            acc[zz] = out[i * 2 * ROWS : (i + 1) * 2 * ROWS].reshape(2, ROWS, 2 * FW)

    def arrivals(s):
        for i in range(2):
            for h, way, hops, nxt in ((i, -1, 4 - i, right), (1 - i, 1, 4 - i, left)):
                if s <= hops:
                    zz = along(way * s)
                    copy4(zz, h, nxt).wait_recv()
                    if s < hops:
                        copy4(zz, h, nxt).start()
                    cross4(zz, h, core).start()

    def other_part(side):
        rows = dot(by_z_s[...], xr[side].reshape(rn, DBI)).astype(BF16)
        acc_b[:, side] = dot(rows, wgu_b[...]).reshape(NZ, ROWS, 2 * FW)

    arrivals(1)
    first_part(z)
    arrivals(2)
    first_part(along(1), along(-1))
    across(0, EARLY, 0)
    arrivals(3)
    across(EARLY, 2 * EARLY, 1)
    first_part(along(2), along(-2))
    across(2 * EARLY, len(ways), 2)
    arrivals(4)
    all_of(wgu_b, lsem.at[4])
    all_of(wdown_a, lsem.at[5])
    all_of(wdown_b, lsem.at[6])
    other_part(core)
    first_part(along(3), along(-3), along(4))
    all_of(xr.at[core], rb2d)
    other_part(other)

    def pair_a(zz):
        return remote(part_a.at[zz, other], rpart_a.at[zz], s5p, r5p.at[zz], mate)

    def finish(*blocks):
        gu = jnp.concatenate([(acc[zz] + acc_b[zz]).reshape(2 * ROWS, 2 * FW) for zz in blocks], axis=0)
        gate, up = jnp.minimum(gu[:, :FW], CLAMP), jnp.clip(gu[:, FW:], -CLAMP, CLAMP)
        act = ((up + 1.0) * (gate * jax.nn.sigmoid(ALPHA * gate))).astype(BF16)
        out = dot(act, wdown_a[...]).astype(BF16)
        for i, zz in enumerate(blocks):
            part_a[zz] = out[2 * i * ROWS : 2 * (i + 1) * ROWS].reshape(2, ROWS, DAO)
            pair_a(zz).start()
        out = dot(act, wdown_b[...]).astype(BF16)
        for i, zz in enumerate(blocks):
            for side in range(2):
                at = (2 * i + side) * ROWS
                part_b[side, zz] = out[at : at + ROWS]
            remote(part_b.at[other, zz], rpart_b.at[zz], sbp, rbp, mate).start()

    def pair_sum(zz, h):
        rows = slice(h * QUARTER, (h + 1) * QUARTER)
        return part_a[zz, core, rows, :].astype(F32) + rpart_a[zz, rows, :].astype(F32)

    def copy5(zz, h, hop, to_right):
        return remote(
            sums.at[zz, h],
            (rright if to_right else rleft).at[h, hop],
            s5,
            (r5r if to_right else r5l).at[h * 4 + hop],
            right if to_right else left,
        )

    def got5(h, hop, from_left):
        return (rright if from_left else rleft)[h, hop].astype(F32)

    def pass_on(hop, h, to_right):
        zz = along(hop if to_right else -hop)
        total = pair_sum(zz, h)
        if hop < (4 - h // 2 if to_right else 3 + h // 2):
            copy5(zz, h, hop, to_right).wait_recv()
            total = total + got5(h, hop, to_right)
        sums[zz, h] = total.astype(BF16)
        copy5(zz, h, hop - 1, to_right).start()

    def pair_sum(zz, h):
        rows = slice(h * QUARTER, (h + 1) * QUARTER)
        return part_a[zz, core, rows, :].astype(F32) + rpart_a[zz, rows, :].astype(F32)

    def copy5(zz, h, hop, to_right):
        return remote(
            sums.at[zz, h],
            (rright if to_right else rleft).at[h, hop],
            s5,
            (r5r if to_right else r5l).at[h * 4 + hop],
            right if to_right else left,
        )

    def got5(h, hop, from_left):
        return (rright if from_left else rleft)[h, hop].astype(F32)

    def pass_on(hop, h, to_right):
        zz = along(hop if to_right else -hop)
        total = pair_sum(zz, h)
        if hop < (4 - h // 2 if to_right else 3 + h // 2):
            copy5(zz, h, hop, to_right).wait_recv()
            total = total + got5(h, hop, to_right)
        sums[zz, h] = total.astype(BF16)
        copy5(zz, h, hop - 1, to_right).start()

    def shorter(hop):
        for h in (0, 1):
            pass_on(hop, h + 2, True)
            pass_on(hop, h, False)

    def longer(hop):
        for h in (0, 1):
            pass_on(hop, h, True)
            pass_on(hop, h + 2, False)

    finish(along(3), along(-3))
    finish(along(4), z)
    pair_a(along(3)).wait_recv()
    pair_a(along(-3)).wait_recv()
    shorter(3)
    finish(along(2), along(-2))
    pair_a(along(4)).wait_recv()
    longer(4)
    finish(along(1), along(-1))
    pair_a(along(2)).wait_recv()
    pair_a(along(-2)).wait_recv()
    shorter(2)

    half_sum = dot(by_a_s[...], part_b[core].reshape(rn, DBO))
    all_of(rpart_b, rbp)
    half_sum = half_sum + dot(by_a_s[...], rpart_b[...].reshape(rn, DBO))
    tb2[...] = half_sum.astype(BF16).reshape(NE, NZ * SLOTS, DBO)
    to_experts(tb2, rr, sb3, rb3)
    rr[ep] = tb2[ep]

    longer(3)
    pair_a(along(1)).wait_recv()
    pair_a(along(-1)).wait_recv()
    shorter(1)
    longer(2)
    longer(1)
    pair_a(z).wait_recv()
    for h in (2, 3, 0, 1):
        total = pair_sum(z, h)
        for to_right in (True, False):
            copy5(z, h, 0, to_right).wait_recv()
            total = total + got5(h, 0, to_right)
        sums[z, h] = total.astype(BF16)

    final = sums[z].astype(F32).reshape(ROWS, DAO).astype(BF16)
    mine = jnp.concatenate([final[:, c * CAO : (c + 1) * CAO] for c in range(NC)], axis=0)
    back = onehot(sr == ((sc // SLOTS) % NE) * 8 + (sc // ROWS) * SLOTS + sc % SLOTS).astype(BF16)
    ob2[...] = dot(back, mine).reshape(NE, 8, CAO).astype(BF16)
    ib2[ep] = ob2[ep]
    to_experts(ob2, ib2, s6, r6)

    def in_two(values):
        high = values.astype(BF16)
        return high, (values - high.astype(F32)).astype(BF16)

    tails = sg[...].reshape(qn, CBI + TAIL)[:, CBI:].astype(F32)
    big_weighed = jnp.zeros(big_q, F32)
    for k in range(4):
        weight = tails[:, k : k + 1] + tails[:, 4 + k : 5 + k]
        big_weighed = big_weighed + onehot(core_ids[:, k : k + 1] == big_e) * weight
    big_high, big_low = in_two(big_chosen * big_weighed)
    all_of(rr.at[pl.ds(0, NE - 1)], rb3)
    taken = rr[...].reshape(rn, DBO)
    mixed = jnp.zeros((qn, CBO), F32)
    for c in range(NC):
        piece = taken[:, c * CBO : (c + 1) * CBO]
        for factor in (big_low, big_high):
            mixed = mixed + dot(jnp.where(c_of_q == c, factor.astype(F32), 0.0).astype(BF16), piece)
    cb[...] = mixed.astype(BF16).reshape(NZ, 16, CBO)
    for d in (4, 3, 5, 2, 6, 1, 7):
        remote(cb.at[along(d)], rcb.at[z], sb4, rb4, at_z(along(d))).start()
    rcb[z] = cb[z]

    high = combine.astype(BF16)
    rest = combine - high.astype(F32)
    middle, lowest = in_two(rest)
    all_of(ib2.at[pl.ds(0, NE - 1)], r6)
    returned = ib2[...].astype(F32).reshape(NE * 8, CAO).astype(BF16)
    mix_a = dot(lowest, returned) + dot(middle, returned) + dot(high, returned)
    all_of(rcb.at[pl.ds(0, NZ - 1)], rb4)
    mix_b = jnp.zeros((16, CBO), F32)
    for zz in range(NZ):
        mix_b = mix_b + rcb[zz].astype(F32)
    tok_s[:, :CAO] = tok_s[:, :CAO] + mix_a
    tok_s[:, CAO:] = tok_s[:, CAO:] + mix_b
    for c in range(NC):
        result_ref[:, c * CW : (c + 1) * CW] = tok_s[c * TOK : (c + 1) * TOK, :].astype(BF16)

    all_of(g1.at[pl.ds(0, NT - 1)], s1)
    pair2.wait_send()
    all_of(sb.at[pl.ds(0, NZ - 1)], s2)
    all_of(sqs.at[pl.ds(0, NZ - 1)], s2q)
    all_of(ob.at[pl.ds(0, NE - 1)], s3)
    all_of(xa.at[pl.ds(0, NZ - 1), 0], s4)
    all_of(xa.at[:, 0], s4d)
    all_of(rpart_a, s5p)
    all_of(sums.at[pl.ds(0, NZ - 1)], s5)
    all_of(ob2.at[pl.ds(0, NE - 1)], s6)
    all_of(sg.at[pl.ds(0, NZ - 1)], sb1)
    all_of(tb.at[pl.ds(0, NE - 1)], sb2)
    all_of(tb, sb2d)
    all_of(rpart_b, sbp)
    all_of(tb2.at[pl.ds(0, NE - 1)], sb3)
    all_of(cb.at[pl.ds(0, NZ - 1)], sb4)


def per_device(
    tokens, rec_state, conv_state, route_ids, route_weights, first_gain, proj_input, proj_gate, conv_taps,
    decay_logit, block_decay, block_input, rec_gain, proj_out, second_gain, expert_gate, expert_up, expert_down,
):
    seqs = rec_state.shape[0]
    vmem, hbm = pl.BlockSpec(memory_space=pltpu.VMEM), pl.BlockSpec(memory_space=pl.ANY)
    dma, v = pltpu.SemaphoreType.DMA, pltpu.VMEM
    result, new_state, new_conv = pl.pallas_call(
        kernel,
        name="layer",
        out_shape=(v(tokens.shape, BF16), v(rec_state.shape, F32), v((3, seqs, W), BF16)),
        in_specs=[hbm] * 18,
        out_specs=(vmem, vmem, vmem),
        scratch_shapes=[
            v(tokens.shape, BF16), v((D // W, W), BF16), v((TOK, seqs), I32), v((TOK, TOK), F32),
            v((seqs, W), F32), v((3, seqs, W), BF16), v((NT, W), F32), v((NT, W), BF16), v((D // W, W), BF16), v((TOK, W), BF16),
            v((D, 2 * W), BF16), v((NC * W, CW), BF16), v((2, W, W), BF16),
            v((DAI, 2 * FW), BF16), v((DBI, 2 * FW), BF16), v((FW, DAO), BF16), v((FW, DBO), BF16),
            v((16, CW), F32), v((NT, 16, CW), BF16),
            v((2, NZ, 16, CW + TAIL), BF16), v((NZ, 16, CW + TAIL), BF16), v((NZ, 16, CW), BF16), v((NZ, 16, CW), BF16),
            v((NZ, 1, TAIL), F32), v((NZ, 1, TAIL), F32),
            v((NE, 8, CAI), BF16), v((NE, 8, CAI), BF16),
            v((NZ, 2, ROWS, DAI), BF16), v((NZ, 2, ROWS, 2 * FW), F32), v((NZ, 2, ROWS, DAO), BF16), v((NZ, ROWS, DAO), BF16),
            v((NZ, 4, QUARTER, DAO), BF16), v((4, 4, QUARTER, DAO), BF16), v((4, 4, QUARTER, DAO), BF16),
            v((NE, 8, CAO), BF16), v((NE, 8, CAO), BF16), v((16, 4), F32),
            v((256, 256), BF16), v((256, 64), BF16), v((256, 256), BF16), v((256, 256), BF16), v((NC, 128, 256), BF16),
            v((NZ, 16, CBI + TAIL), BF16), v((NE, 16, DBI), BF16), v((2, NE, 16, DBI), BF16), v((NZ, 2, ROWS, 2 * FW), F32),
            v((2, NZ, ROWS, DBO), BF16), v((NZ, ROWS, DBO), BF16), v((NE, 16, DBO), BF16), v((NE, 16, DBO), BF16),
            v((NZ, 16, CBO), BF16), v((NZ, 16, CBO), BF16),
            dma((17,)), dma, dma, dma, dma((NZ + 1,)), dma, dma, dma, dma, dma, dma,
            dma, dma((NZ * 2,)), dma, dma((NZ,)), dma, dma((NZ,)), dma, dma((16,)), dma((16,)), dma, dma,
            dma, dma, dma, dma((3,)), dma, dma, dma, dma, dma, dma, dma, dma,
        ],
        compiler_params=pltpu.CompilerParams(
            collective_id=0, has_side_effects=True, vmem_limit_bytes=60 * 1024 * 1024
        ),
    )(
        tokens, first_gain.reshape(D // W, W), route_ids.T, route_weights, rec_state, conv_state.transpose(1, 0, 2),
        decay_logit.reshape(NT, W), rec_gain.reshape(NT, W), second_gain.reshape(D // W, W), conv_taps,
        proj_input, proj_gate, block_decay, block_input, proj_out, expert_gate, expert_up, expert_down,
    )
    def store(a_ref, b_ref, c_ref, a_hbm, b_hbm, c_hbm, sem):
        copies = [
            pltpu.make_async_copy(src, dst, sem.at[i])
            for i, (src, dst) in enumerate(((a_ref, a_hbm), (b_ref, b_hbm), (c_ref, c_hbm)))
        ]
        for copy in copies:
            copy.start()
        for copy in copies:
            copy.wait()

    outs = tuple(pltpu.with_memory_space_constraint(o, pltpu.VMEM) for o in (result, new_state, new_conv))
    result, new_state, new_conv = pl.pallas_call(
        store,
        name="store",
        out_shape=tuple(jax.ShapeDtypeStruct(o.shape, o.dtype) for o in outs),
        in_specs=[vmem] * 3,
        out_specs=(hbm,) * 3,
        scratch_shapes=[dma((3,))],
    )(*outs)
    return result, new_state, new_conv.transpose(1, 0, 2)


def solution(mesh):
    in_specs = (
        P(("ep", "tp"), None),
        P("ep", "tp"),
        P("ep", None, "tp"),
        P("ep", None),
        P(("ep", "tp"), None),
        P(),
        P(None, "tp"),
        P(None, "tp"),
        P(),
        P(),
        P(),
        P(),
        P(),
        P("tp", None),
        P(),
        P("ep", None, "tp"),
        P("ep", None, "tp"),
        P("ep", "tp", None),
    )
    out_specs = (P(("ep", "tp"), None), P("ep", "tp"), P("ep", None, "tp"))
    return jax.shard_map(
        per_device, mesh=mesh, in_specs=in_specs, out_specs=out_specs, check_vma=False
    )
```

```python
import jax
import jax.numpy as jnp
from jax import lax
from jax.experimental import pallas as pl
from jax.experimental.pallas import tpu as pltpu
from jax.sharding import PartitionSpec as P

MESH = pl.DeviceIdType.MESH
BF16, F32, I32 = jnp.bfloat16, jnp.float32, jnp.int32

EPS = 1e-06
CLAMP = 7.0
ALPHA = 1.702
RATE = 8.0

D = 4096
NC = 4
CW = D // NC
TOK = 4
NE = 16
NT = 16
NZ = 8
D_REC = 2048
W = 128
FW = 256
SLOTS = 2
ROWS = NE * SLOTS
HALF = ROWS // 2
QUARTER = ROWS // 4
TAIL = 128
EARLY = 5
CBI, CBO = 512, 384
CAI, CAO = CW - CBI, CW - CBO
DAI, DBI, DAO, DBO = NC * CAI, NC * CBI, NC * CAO, NC * CBO


def iota(shape, dim):
    return lax.broadcasted_iota(I32, shape, dim)


def onehot(cond):
    return jnp.where(cond, 1.0, 0.0).astype(F32)


def dot(a, b):
    return jnp.dot(a, b, preferred_element_type=F32)


def per_token(values):
    part = jnp.broadcast_to(jnp.sum(values, axis=1, keepdims=True), (NC * TOK, 128))
    total = part
    for c in range(1, NC):
        total = total + pltpu.roll(part, c * TOK, 0)
    return total[:, 0:1]


def spread(ref):
    values, shape = ref[...].astype(F32), (NC * TOK, 128)
    c_of = iota(shape, 0) // TOK
    blocks = []
    for i in range(CW // 128):
        block = jnp.broadcast_to(values[i : i + 1, :], shape)
        for c in range(1, NC):
            row = c * (CW // 128) + i
            block = jnp.where(c_of == c, jnp.broadcast_to(values[row : row + 1, :], shape), block)
        blocks.append(block)
    return jnp.concatenate(blocks, axis=1)


def minus_expm1(x):
    small = jnp.full_like(x, 1.0)
    for k in range(8, 1, -1):
        small = 1.0 + small * x * (1.0 / k)
    return jnp.where(x > -0.3, -x * small, 1.0 - jnp.exp(x))


def kernel(
    tokens_hbm, gain1_hbm, ids_hbm, weights_hbm, rec_hbm, conv_hbm, logit_hbm, rgain_hbm, gain2_hbm, taps_hbm,
    pin_hbm, pgate_hbm, bdec_hbm, binp_hbm, pout_hbm, eg_hbm, eu_hbm, ed_hbm,
    result_ref, state_ref, newconv_ref,
    tokens_ref, gain1_ref, ids_ref, weights_ref, rec_ref, conv_ref, logit_ref, rgain_ref, gain2_ref, taps_ref,
    wcat, w4, gates, wgu_a, wgu_b, wdown_a, wdown_b,
    tok_s, g1, pb, rp, sb, rb, sqs, sqr, ob, ib, xa, acc, part_a, rpart_a, sums, rright, rleft, ob2, ib2, rw_s,
    perm_s, expand_s, by_z_s, by_a_s, chosen_s,
    sg, tb, xr, acc_b, part_b, rpart_b, tb2, rr, cb, rcb,
    lsem, s1, s2q, r2q, r1, s2p, r2p, s2, r2, s3, r3, s4, r4, s4d, r4d, s5p, r5p, s5, r5r, r5l, s6, r6,
    sb1, rb1, sb2, rb2, sb2d, rb2d, sbp, rbp, sb3, rb3, sb4, rb4,
):
    ep = lax.axis_index("ep")
    tp = lax.axis_index("tp")
    z = tp // 2
    core = tp % 2
    other = 1 - core
    mate = (ep, z * 2 + other)
    y, x = ep // 4, ep % 4

    def remote(src, dst, ss, rs, dev):
        return pltpu.make_async_remote_copy(
            src_ref=src, dst_ref=dst, send_sem=ss, recv_sem=rs, device_id=dev, device_id_type=MESH
        )

    def all_of(ref, sem):
        pltpu.make_async_copy(ref, ref, sem).wait()

    def over(dy, dx):
        return ((y + dy + 4) % 4) * 4 + (x + dx + 4) % 4

    def along(d):
        return (z + d + NZ) % NZ

    def at_z(zz):
        return (ep, zz * 2 + core)

    barrier = pltpu.get_barrier_semaphore()
    pl.semaphore_signal(barrier, inc=1, device_id=mate, device_id_type=MESH)
    for d in range(1, NZ):
        pl.semaphore_signal(barrier, inc=1, device_id=at_z(along(d)), device_id_type=MESH)
    for d in range(1, NE):
        pl.semaphore_signal(barrier, inc=1, device_id=((ep + d) % NE, tp), device_id_type=MESH)

    smalls = [
        pltpu.make_async_copy(src, dst, lsem.at[7 + i])
        for i, (src, dst) in enumerate((
            (tokens_hbm, tokens_ref), (gain1_hbm, gain1_ref), (ids_hbm, ids_ref), (weights_hbm, weights_ref),
            (rec_hbm, rec_ref), (conv_hbm, conv_ref), (logit_hbm, logit_ref), (rgain_hbm, rgain_ref),
            (gain2_hbm, gain2_ref), (taps_hbm.at[:, pl.ds(pl.multiple_of(tp * W, W), W)], taps_ref),
        ))
    ]
    for load in smalls:
        load.start()
    loads = [
        pltpu.make_async_copy(pin_hbm, wcat.at[:, pl.ds(0, W)], lsem.at[0]),
        pltpu.make_async_copy(pgate_hbm, wcat.at[:, pl.ds(W, W)], lsem.at[0]),
        pltpu.make_async_copy(bdec_hbm.at[tp], gates.at[0], lsem.at[1]),
        pltpu.make_async_copy(binp_hbm.at[tp], gates.at[1], lsem.at[1]),
    ]
    for c in range(NC):
        loads.append(
            pltpu.make_async_copy(
                pout_hbm.at[:, pl.ds(c * CW, CW)], w4.at[pl.ds(c * W, W), :], lsem.at[2]
            )
        )
    for load in loads:
        load.start()
    for c in range(NC):
        for i, (hbm, col) in enumerate(((eg_hbm, 0), (eu_hbm, FW))):
            for dst, first, size, sem in ((wgu_a, 0, CAI, 3), (wgu_b, CAI, CBI, 4)):
                pltpu.make_async_copy(
                    hbm.at[0, pl.ds(c * CW + first, size), :],
                    dst.at[pl.ds(c * size, size), pl.ds(col, FW)],
                    lsem.at[sem],
                ).start()
        for dst, first, size, sem in ((wdown_a, 0, CAO, 5), (wdown_b, CAO, CBO, 6)):
            pltpu.make_async_copy(
                ed_hbm.at[0, :, pl.ds(c * CW + first, size)], dst.at[:, pl.ds(c * size, size)], lsem.at[sem]
            ).start()

    smalls[0].wait()
    smalls[1].wait()
    own = tokens_ref[...].astype(F32)
    for c in range(NC):
        tok_s[c * TOK : (c + 1) * TOK, :] = own[:, c * CW : (c + 1) * CW]
    values = tok_s[...]
    scale = lax.rsqrt(per_token(values * values) * (1.0 / D) + EPS)
    g1[tp] = (values * scale * spread(gain1_ref)).astype(BF16)

    pl.semaphore_wait(barrier, NZ + NE - 1)

    for d in (4, 3, 5, 2, 6, 1, 7):
        remote(g1.at[tp], g1.at[tp], s1, r1.at[z], at_z(along(d))).start()
    remote(g1.at[tp], g1.at[tp], s1, r1.at[NZ], mate).start()

    q4, r4e = (NC * TOK, W), 8
    row_n, row_c = iota(q4, 0) % TOK, iota(q4, 0) // TOK
    lane_e, lane_c, lane_s = iota(q4, 1) // r4e, (iota(q4, 1) // SLOTS) % NC, iota(q4, 1) % SLOTS
    pick_own = onehot(iota((NC * TOK, NE * TOK), 1) == tp * TOK + iota((NC * TOK, NE * TOK), 0) % TOK)
    smalls[2].wait()
    smalls[3].wait()
    all_ids = ids_ref[...].astype(F32).astype(BF16)
    own_ids = lax.dot_general(pick_own.astype(BF16), all_ids, (((1,), (1,)), ((), ())), preferred_element_type=F32)
    for c in range(NC):
        rw_s[c * TOK : (c + 1) * TOK, :] = weights_ref[...]
    hit = jnp.zeros(q4, F32)
    weighed = jnp.zeros(q4, F32)
    lane_ef = lane_e.astype(F32)
    for k in range(4):
        same = onehot(own_ids[:, k : k + 1] == lane_ef)
        hit = hit + same
        weighed = weighed + same * rw_s[:, k : k + 1]
    sq = (NC * TOK, NC * TOK)
    earlier = onehot(
        (iota(sq, 0) // TOK == iota(sq, 1) // TOK) & (iota(sq, 1) % TOK < iota(sq, 0) % TOK)
    )
    before = dot(earlier.astype(BF16), hit.astype(BF16))
    chosen = hit * onehot((before == lane_s.astype(F32)) & (row_c == lane_c))
    combine = chosen * weighed

    qn, rn = NZ * NC * TOK, NE * NZ * SLOTS
    big_q = (qn, rn)
    pick_core = onehot(
        iota((qn, NE * TOK), 1) == ((iota((qn, NE * TOK), 0) // 16) * 2 + core) * TOK + iota((qn, NE * TOK), 0) % TOK
    )
    core_ids = lax.dot_general(pick_core.astype(BF16), all_ids, (((1,), (1,)), ((), ())), preferred_element_type=F32)
    big_e = (iota(big_q, 1) // (NZ * SLOTS)).astype(F32)
    big_s = (iota(big_q, 1) % SLOTS).astype(F32)
    same_z = iota(big_q, 0) // 16 == (iota(big_q, 1) // SLOTS) % NZ
    big_hit = jnp.zeros(big_q, F32)
    for k in range(4):
        big_hit = big_hit + onehot(core_ids[:, k : k + 1] == big_e)
    qq = (qn, qn)
    big_earlier = onehot(
        (iota(qq, 0) // TOK == iota(qq, 1) // TOK) & (iota(qq, 1) % TOK < iota(qq, 0) % TOK)
    )
    big_before = dot(big_earlier.astype(BF16), big_hit.astype(BF16))
    big_chosen = big_hit * onehot((big_before == big_s) & same_z)
    c_of_q = (iota(big_q, 0) // TOK) % NC
    for c in range(NC):
        chosen_s[c] = jnp.where(c_of_q == c, big_chosen, 0.0).astype(BF16)

    big = NT * NC * TOK
    pr, pc = iota((big, big), 0), iota((big, big), 1)
    perm_s[...] = onehot(pc == ((pr // TOK) % NT) * 16 + (pr // 64) * TOK + pr % TOK).astype(BF16)
    er, et = iota((big, NT * TOK), 0), iota((big, NT * TOK), 1)
    expand_s[...] = onehot(et == (((er // 16) % NZ) * 2 + er // 128) * TOK + er % TOK).astype(BF16)
    tr, tc = iota((rn, rn), 0), iota((rn, rn), 1)
    by_z_s[...] = onehot(tc == ((tr // SLOTS) % NE) * 16 + (tr // ROWS) * SLOTS + tr % SLOTS).astype(BF16)
    by_a_s[...] = onehot(tr == ((tc // SLOTS) % NE) * 16 + (tc // ROWS) * SLOTS + tc % SLOTS).astype(BF16)

    for d in (1, 7, 2, 6, 3, 5, 4):
        zz = along(d)
        block = g1.at[zz * 2 + core]
        remote(block, block, s1, r1.at[zz], mate).wait_recv()
        remote(block, block, s1, r1.at[NZ], mate).start()
    all_of(g1.at[pl.ds(0, NZ)], r1.at[NZ])

    stacked = dot(perm_s[...], g1[...].reshape(big, CW)).astype(BF16)
    for load in smalls[4:]:
        load.wait()
    all_of(wcat, lsem.at[0])
    all_of(gates, lsem.at[1])
    both = jnp.zeros((NT * TOK, 2 * W), F32)
    for c in range(NC):
        both = both + dot(stacked[c * 64 : (c + 1) * 64, :], wcat[c * CW : (c + 1) * CW, :])
    joined = both.astype(BF16)
    branch_in, branch_gate = joined[:, :W].astype(F32), joined[:, W:].astype(F32)

    taps = taps_ref[...].astype(F32)
    conv = taps[3:4, :] * branch_in
    for tap in range(3):
        conv = conv + taps[tap : tap + 1, :] * conv_ref[tap].astype(F32)
    newconv_ref[0:2] = conv_ref[1:3]
    newconv_ref[2] = joined[:, :W]

    low = conv.astype(BF16)
    decay_gate = jax.nn.sigmoid(dot(low, gates[0]))
    input_gate = jax.nn.sigmoid(dot(low, gates[1]))
    mine = iota((NT, W), 0) == tp
    logit = jnp.sum(jnp.where(mine, logit_ref[...], 0.0), axis=0, keepdims=True)
    rgain = jnp.sum(jnp.where(mine, rgain_ref[...].astype(F32), 0.0), axis=0, keepdims=True)
    soft = jnp.maximum(-logit, 0.0) + jnp.log1p(jnp.exp(-jnp.abs(logit)))
    log_keep = -RATE * decay_gate * soft
    new_state = jnp.exp(log_keep) * rec_ref[...] + jnp.sqrt(minus_expm1(2.0 * log_keep)) * input_gate * conv
    state_ref[...] = new_state
    hidden = new_state * jax.nn.gelu(branch_gate)
    squares = jnp.broadcast_to(jnp.sum(hidden * hidden, axis=1, keepdims=True), (NT * TOK, W))

    wide = dot(expand_s[...], jnp.concatenate([(hidden * rgain).astype(BF16), squares.astype(BF16)], axis=1))
    gained, sq_wide = wide[:, :W], wide[:, W:]
    c_of = (iota((big, W), 0) // TOK) % NC
    all_of(w4, lsem.at[2])
    lhs = jnp.concatenate([jnp.where(c_of == c, gained, 0.0) for c in range(NC)], axis=1).astype(BF16)
    pb[:, :, :, 0:CW] = dot(lhs, w4[...]).astype(BF16).reshape(2, NZ, 16, CW)
    pb[:, :, :, CW : CW + TAIL] = sq_wide.astype(BF16).reshape(2, NZ, 16, TAIL)

    pair2 = pltpu.make_async_remote_copy(
        src_ref=pb.at[other], dst_ref=rp, send_sem=s2p, recv_sem=r2p, device_id=mate, device_id_type=MESH
    )
    pair2.start()
    pair2.wait_recv()

    row_of, lane_of = iota((NC * TOK, TAIL), 0), iota((NC * TOK, TAIL), 1)

    def in_a_row(zz):
        total = pb[core, zz, :, CW:].astype(F32) + rp[zz, :, CW:].astype(F32)
        return jnp.sum(jnp.where(row_of == lane_of, total, 0.0), axis=0, keepdims=True)

    for d in (4, 3, 5, 2, 6, 1, 7):
        zz = along(d)
        sb[zz] = (pb[core, zz, :, :CW].astype(F32) + rp[zz, :, :CW].astype(F32)).astype(BF16)
        sqs[zz] = in_a_row(zz)
        remote(sqs.at[zz], sqr.at[z], s2q, r2q, at_z(zz)).start()
        remote(sb.at[zz], rb.at[z], s2, r2, at_z(zz)).start()
    sqr[z] = in_a_row(z)
    rb[z] = (pb[core, z, :, :CW].astype(F32) + rp[z, :, :CW].astype(F32)).astype(BF16)
    all_of(sqr.at[pl.ds(0, NZ - 1)], r2q)
    own_row = sqr[0]
    for zz in range(1, NZ):
        own_row = own_row + sqr[zz]
    own_squares = jnp.sum(
        jnp.where(row_of == lane_of, jnp.broadcast_to(own_row, (NC * TOK, TAIL)), 0.0), axis=1, keepdims=True
    )
    all_of(rb.at[pl.ds(0, NZ - 1)], r2)
    summed = jnp.zeros((16, CW), F32)
    for zz in range(NZ):
        summed = summed + rb[zz].astype(F32)
    residual = tok_s[...] + summed * lax.rsqrt(own_squares * (1.0 / D_REC) + EPS)
    scale = lax.rsqrt(per_token(residual * residual) * (1.0 / D) + EPS)
    second = (residual * scale * spread(gain2_ref)).astype(BF16)
    tok_s[...] = residual

    w_high = rw_s[...].astype(BF16).astype(F32)
    w_rest = rw_s[...] - w_high
    lane = iota((NC * TOK, TAIL), 1)
    tail = jnp.zeros((NC * TOK, TAIL), F32)
    for k in range(4):
        tail = jnp.where(lane == k, w_high[:, k : k + 1], tail)
        tail = jnp.where(lane == 4 + k, w_rest[:, k : k + 1], tail)
    sg[z, :, 0:CBI] = second[:, CAI:]
    sg[z, :, CBI:] = tail.astype(BF16)
    sent = lax.dot_general(
        chosen.astype(BF16), second[:, :CAI], (((0,), (0,)), ((), ())), preferred_element_type=F32
    )
    ob[...] = sent.reshape(NE, 8, CAI).astype(BF16)
    ib[ep] = ob[ep]
    for d in (4, 3, 5, 2, 6, 1, 7):
        remote(sg.at[z], sg.at[z], sb1, rb1, at_z(along(d))).start()

    ways = (
        (2, 2), (2, 1), (1, 3), (3, 2), (0, 2), (2, 3), (1, 2), (2, 0),
        (3, 1), (3, 3), (1, 1), (0, 3), (1, 0), (0, 1), (3, 0),
    )

    def to_experts(src, dst, ss, rs):
        for dy, dx in ways:
            e = over(dy, dx)
            remote(src.at[e], dst.at[ep], ss, rs, (e, tp)).start()

    to_experts(ob, ib, s3, r3)

    all_of(ib.at[pl.ds(0, NE - 1)], r3)
    own_rows = NE * 8
    sr, sc = iota((own_rows, own_rows), 0), iota((own_rows, own_rows), 1)
    turn = onehot(sc == ((sr // SLOTS) % NE) * 8 + (sr // ROWS) * SLOTS + sr % SLOTS).astype(BF16)
    turned = dot(turn, ib[...].astype(F32).reshape(own_rows, CAI).astype(BF16)).astype(BF16)
    for c in range(NC):
        xa[z, core, :, c * CAI : (c + 1) * CAI] = turned[c * ROWS : (c + 1) * ROWS, :]

    def copy4(zz, h, dev):
        block = xa.at[zz, core, pl.ds(h * HALF, HALF), :]
        return remote(block, block, s4, r4.at[zz * 2 + h], dev)

    def cross4(zz, h, side):
        block = xa.at[zz, side, pl.ds(h * HALF, HALF), :]
        return remote(block, block, s4d, r4d.at[zz], mate)

    right, left = at_z(along(1)), at_z(along(-1))
    for h in range(2):
        copy4(z, h, right).start()
        copy4(z, 1 - h, left).start()
    cross4(z, 0, core).start()
    cross4(z, 1, core).start()

    all_of(sg.at[pl.ds(0, NZ - 1)], rb1)
    group = sg[...].reshape(qn, CBI + TAIL)
    for c in range(NC):
        picked = lax.dot_general(
            chosen_s[c], group[:, :CBI], (((0,), (0,)), ((), ())), preferred_element_type=F32
        )
        tb[:, :, c * CBI : (c + 1) * CBI] = picked.reshape(NE, NZ * SLOTS, CBI).astype(BF16)
    for i, (dy, dx) in enumerate(ways):
        e = over(dy, dx)
        remote(tb.at[e], xr.at[core, ep], sb2, rb2.at[min(i // EARLY, 2)], (e, tp)).start()
    xr[core, ep] = tb[ep]
    remote(tb.at[ep], xr.at[core, ep], sb2d, rb2d, mate).start()

    def across(first, last, group):
        all_of(tb.at[pl.ds(0, last - first)], rb2.at[group])
        for dy, dx in ways[first:last]:
            source = over(-dy, -dx)
            block = xr.at[core, source]
            remote(block, block, sb2d, rb2d, mate).start()

    all_of(wgu_a, lsem.at[3])

    def first_part(*blocks):
        for zz in blocks:
            all_of(xa.at[zz, other], r4d.at[zz])
        rows = jnp.concatenate([xa[zz].reshape(2 * ROWS, DAI) for zz in blocks], axis=0)
        out = dot(rows, wgu_a[...])
        for i, zz in enumerate(blocks):
            acc[zz] = out[i * 2 * ROWS : (i + 1) * 2 * ROWS].reshape(2, ROWS, 2 * FW)

    def arrivals(s):
        for i in range(2):
            for h, way, hops, nxt in ((i, -1, 4 - i, right), (1 - i, 1, 4 - i, left)):
                if s <= hops:
                    zz = along(way * s)
                    copy4(zz, h, nxt).wait_recv()
                    if s < hops:
                        copy4(zz, h, nxt).start()
                    cross4(zz, h, core).start()

    def other_part(side):
        rows = dot(by_z_s[...], xr[side].reshape(rn, DBI)).astype(BF16)
        acc_b[:, side] = dot(rows, wgu_b[...]).reshape(NZ, ROWS, 2 * FW)

    arrivals(1)
    first_part(z)
    arrivals(2)
    first_part(along(1), along(-1))
    across(0, EARLY, 0)
    arrivals(3)
    across(EARLY, 2 * EARLY, 1)
    first_part(along(2), along(-2))
    across(2 * EARLY, len(ways), 2)
    arrivals(4)
    all_of(wgu_b, lsem.at[4])
    all_of(wdown_a, lsem.at[5])
    all_of(wdown_b, lsem.at[6])
    other_part(core)
    first_part(along(3), along(-3), along(4))
    all_of(xr.at[core], rb2d)
    other_part(other)

    def pair_a(zz):
        return remote(part_a.at[zz, other], rpart_a.at[zz], s5p, r5p.at[zz], mate)

    def finish(*blocks):
        gu = jnp.concatenate([(acc[zz] + acc_b[zz]).reshape(2 * ROWS, 2 * FW) for zz in blocks], axis=0)
        gate, up = jnp.minimum(gu[:, :FW], CLAMP), jnp.clip(gu[:, FW:], -CLAMP, CLAMP)
        act = ((up + 1.0) * (gate * jax.nn.sigmoid(ALPHA * gate))).astype(BF16)
        out = dot(act, wdown_a[...]).astype(BF16)
        for i, zz in enumerate(blocks):
            part_a[zz] = out[2 * i * ROWS : 2 * (i + 1) * ROWS].reshape(2, ROWS, DAO)
            pair_a(zz).start()
        out = dot(act, wdown_b[...]).astype(BF16)
        for i, zz in enumerate(blocks):
            for side in range(2):
                at = (2 * i + side) * ROWS
                part_b[side, zz] = out[at : at + ROWS]
            remote(part_b.at[other, zz], rpart_b.at[zz], sbp, rbp, mate).start()

    def pair_sum(zz, h):
        rows = slice(h * QUARTER, (h + 1) * QUARTER)
        return part_a[zz, core, rows, :].astype(F32) + rpart_a[zz, rows, :].astype(F32)

    def copy5(zz, h, hop, to_right):
        return remote(
            sums.at[zz, h],
            (rright if to_right else rleft).at[h, hop],
            s5,
            (r5r if to_right else r5l).at[h * 4 + hop],
            right if to_right else left,
        )

    def got5(h, hop, from_left):
        return (rright if from_left else rleft)[h, hop].astype(F32)

    def pass_on(hop, h, to_right):
        zz = along(hop if to_right else -hop)
        total = pair_sum(zz, h)
        if hop < (4 - h // 2 if to_right else 3 + h // 2):
            copy5(zz, h, hop, to_right).wait_recv()
            total = total + got5(h, hop, to_right)
        sums[zz, h] = total.astype(BF16)
        copy5(zz, h, hop - 1, to_right).start()

    def pair_sum(zz, h):
        rows = slice(h * QUARTER, (h + 1) * QUARTER)
        return part_a[zz, core, rows, :].astype(F32) + rpart_a[zz, rows, :].astype(F32)

    def copy5(zz, h, hop, to_right):
        return remote(
            sums.at[zz, h],
            (rright if to_right else rleft).at[h, hop],
            s5,
            (r5r if to_right else r5l).at[h * 4 + hop],
            right if to_right else left,
        )

    def got5(h, hop, from_left):
        return (rright if from_left else rleft)[h, hop].astype(F32)

    def pass_on(hop, h, to_right):
        zz = along(hop if to_right else -hop)
        total = pair_sum(zz, h)
        if hop < (4 - h // 2 if to_right else 3 + h // 2):
            copy5(zz, h, hop, to_right).wait_recv()
            total = total + got5(h, hop, to_right)
        sums[zz, h] = total.astype(BF16)
        copy5(zz, h, hop - 1, to_right).start()

    def shorter(hop):
        for h in (0, 1):
            pass_on(hop, h + 2, True)
            pass_on(hop, h, False)

    def longer(hop):
        for h in (0, 1):
            pass_on(hop, h, True)
            pass_on(hop, h + 2, False)

    finish(along(4), z)
    finish(along(3), along(-3))
    pair_a(along(4)).wait_recv()
    longer(4)
    finish(along(2), along(-2))
    pair_a(along(3)).wait_recv()
    pair_a(along(-3)).wait_recv()
    shorter(3)
    finish(along(1), along(-1))

    half_sum = dot(by_a_s[...], part_b[core].reshape(rn, DBO))
    all_of(rpart_b, rbp)
    half_sum = half_sum + dot(by_a_s[...], rpart_b[...].reshape(rn, DBO))
    tb2[...] = half_sum.astype(BF16).reshape(NE, NZ * SLOTS, DBO)
    to_experts(tb2, rr, sb3, rb3)
    rr[ep] = tb2[ep]

    longer(3)
    pair_a(along(2)).wait_recv()
    pair_a(along(-2)).wait_recv()
    shorter(2)
    longer(2)
    pair_a(along(1)).wait_recv()
    pair_a(along(-1)).wait_recv()
    shorter(1)
    longer(1)
    pair_a(z).wait_recv()
    for h in (2, 3, 0, 1):
        total = pair_sum(z, h)
        for to_right in (True, False):
            copy5(z, h, 0, to_right).wait_recv()
            total = total + got5(h, 0, to_right)
        sums[z, h] = total.astype(BF16)

    final = sums[z].astype(F32).reshape(ROWS, DAO).astype(BF16)
    mine = jnp.concatenate([final[:, c * CAO : (c + 1) * CAO] for c in range(NC)], axis=0)
    back = onehot(sr == ((sc // SLOTS) % NE) * 8 + (sc // ROWS) * SLOTS + sc % SLOTS).astype(BF16)
    ob2[...] = dot(back, mine).reshape(NE, 8, CAO).astype(BF16)
    ib2[ep] = ob2[ep]
    to_experts(ob2, ib2, s6, r6)

    def in_two(values):
        high = values.astype(BF16)
        return high, (values - high.astype(F32)).astype(BF16)

    tails = sg[...].reshape(qn, CBI + TAIL)[:, CBI:].astype(F32)
    big_weighed = jnp.zeros(big_q, F32)
    for k in range(4):
        weight = tails[:, k : k + 1] + tails[:, 4 + k : 5 + k]
        big_weighed = big_weighed + onehot(core_ids[:, k : k + 1] == big_e) * weight
    big_high, big_low = in_two(big_chosen * big_weighed)
    all_of(rr.at[pl.ds(0, NE - 1)], rb3)
    taken = rr[...].reshape(rn, DBO)
    mixed = jnp.zeros((qn, CBO), F32)
    for c in range(NC):
        piece = taken[:, c * CBO : (c + 1) * CBO]
        for factor in (big_low, big_high):
            mixed = mixed + dot(jnp.where(c_of_q == c, factor.astype(F32), 0.0).astype(BF16), piece)
    cb[...] = mixed.astype(BF16).reshape(NZ, 16, CBO)
    for d in (4, 3, 5, 2, 6, 1, 7):
        remote(cb.at[along(d)], rcb.at[z], sb4, rb4, at_z(along(d))).start()
    rcb[z] = cb[z]

    high = combine.astype(BF16)
    rest = combine - high.astype(F32)
    middle, lowest = in_two(rest)
    all_of(ib2.at[pl.ds(0, NE - 1)], r6)
    returned = ib2[...].astype(F32).reshape(NE * 8, CAO).astype(BF16)
    mix_a = dot(lowest, returned) + dot(middle, returned) + dot(high, returned)
    all_of(rcb.at[pl.ds(0, NZ - 1)], rb4)
    mix_b = jnp.zeros((16, CBO), F32)
    for zz in range(NZ):
        mix_b = mix_b + rcb[zz].astype(F32)
    tok_s[:, :CAO] = tok_s[:, :CAO] + mix_a
    tok_s[:, CAO:] = tok_s[:, CAO:] + mix_b
    for c in range(NC):
        result_ref[:, c * CW : (c + 1) * CW] = tok_s[c * TOK : (c + 1) * TOK, :].astype(BF16)

    all_of(g1.at[pl.ds(0, NT - 1)], s1)
    pair2.wait_send()
    all_of(sb.at[pl.ds(0, NZ - 1)], s2)
    all_of(sqs.at[pl.ds(0, NZ - 1)], s2q)
    all_of(ob.at[pl.ds(0, NE - 1)], s3)
    all_of(xa.at[pl.ds(0, NZ - 1), 0], s4)
    all_of(xa.at[:, 0], s4d)
    all_of(rpart_a, s5p)
    all_of(sums.at[pl.ds(0, NZ - 1)], s5)
    all_of(ob2.at[pl.ds(0, NE - 1)], s6)
    all_of(sg.at[pl.ds(0, NZ - 1)], sb1)
    all_of(tb.at[pl.ds(0, NE - 1)], sb2)
    all_of(tb, sb2d)
    all_of(rpart_b, sbp)
    all_of(tb2.at[pl.ds(0, NE - 1)], sb3)
    all_of(cb.at[pl.ds(0, NZ - 1)], sb4)


def per_device(
    tokens, rec_state, conv_state, route_ids, route_weights, first_gain, proj_input, proj_gate, conv_taps,
    decay_logit, block_decay, block_input, rec_gain, proj_out, second_gain, expert_gate, expert_up, expert_down,
):
    seqs = rec_state.shape[0]
    vmem, hbm = pl.BlockSpec(memory_space=pltpu.VMEM), pl.BlockSpec(memory_space=pl.ANY)
    dma, v = pltpu.SemaphoreType.DMA, pltpu.VMEM
    result, new_state, new_conv = pl.pallas_call(
        kernel,
        name="layer",
        out_shape=(v(tokens.shape, BF16), v(rec_state.shape, F32), v((3, seqs, W), BF16)),
        in_specs=[hbm] * 18,
        out_specs=(vmem, vmem, vmem),
        scratch_shapes=[
            v(tokens.shape, BF16), v((D // W, W), BF16), v((TOK, seqs), I32), v((TOK, TOK), F32),
            v((seqs, W), F32), v((3, seqs, W), BF16), v((NT, W), F32), v((NT, W), BF16), v((D // W, W), BF16), v((TOK, W), BF16),
            v((D, 2 * W), BF16), v((NC * W, CW), BF16), v((2, W, W), BF16),
            v((DAI, 2 * FW), BF16), v((DBI, 2 * FW), BF16), v((FW, DAO), BF16), v((FW, DBO), BF16),
            v((16, CW), F32), v((NT, 16, CW), BF16),
            v((2, NZ, 16, CW + TAIL), BF16), v((NZ, 16, CW + TAIL), BF16), v((NZ, 16, CW), BF16), v((NZ, 16, CW), BF16),
            v((NZ, 1, TAIL), F32), v((NZ, 1, TAIL), F32),
            v((NE, 8, CAI), BF16), v((NE, 8, CAI), BF16),
            v((NZ, 2, ROWS, DAI), BF16), v((NZ, 2, ROWS, 2 * FW), F32), v((NZ, 2, ROWS, DAO), BF16), v((NZ, ROWS, DAO), BF16),
            v((NZ, 4, QUARTER, DAO), BF16), v((4, 4, QUARTER, DAO), BF16), v((4, 4, QUARTER, DAO), BF16),
            v((NE, 8, CAO), BF16), v((NE, 8, CAO), BF16), v((16, 4), F32),
            v((256, 256), BF16), v((256, 64), BF16), v((256, 256), BF16), v((256, 256), BF16), v((NC, 128, 256), BF16),
            v((NZ, 16, CBI + TAIL), BF16), v((NE, 16, DBI), BF16), v((2, NE, 16, DBI), BF16), v((NZ, 2, ROWS, 2 * FW), F32),
            v((2, NZ, ROWS, DBO), BF16), v((NZ, ROWS, DBO), BF16), v((NE, 16, DBO), BF16), v((NE, 16, DBO), BF16),
            v((NZ, 16, CBO), BF16), v((NZ, 16, CBO), BF16),
            dma((17,)), dma, dma, dma, dma((NZ + 1,)), dma, dma, dma, dma, dma, dma,
            dma, dma((NZ * 2,)), dma, dma((NZ,)), dma, dma((NZ,)), dma, dma((16,)), dma((16,)), dma, dma,
            dma, dma, dma, dma((3,)), dma, dma, dma, dma, dma, dma, dma, dma,
        ],
        compiler_params=pltpu.CompilerParams(
            collective_id=0, has_side_effects=True, vmem_limit_bytes=60 * 1024 * 1024
        ),
    )(
        tokens, first_gain.reshape(D // W, W), route_ids.T, route_weights, rec_state, conv_state.transpose(1, 0, 2),
        decay_logit.reshape(NT, W), rec_gain.reshape(NT, W), second_gain.reshape(D // W, W), conv_taps,
        proj_input, proj_gate, block_decay, block_input, proj_out, expert_gate, expert_up, expert_down,
    )
    def store(a_ref, b_ref, c_ref, a_hbm, b_hbm, c_hbm, sem):
        copies = [
            pltpu.make_async_copy(src, dst, sem.at[i])
            for i, (src, dst) in enumerate(((a_ref, a_hbm), (b_ref, b_hbm), (c_ref, c_hbm)))
        ]
        for copy in copies:
            copy.start()
        for copy in copies:
            copy.wait()

    outs = tuple(pltpu.with_memory_space_constraint(o, pltpu.VMEM) for o in (result, new_state, new_conv))
    result, new_state, new_conv = pl.pallas_call(
        store,
        name="store",
        out_shape=tuple(jax.ShapeDtypeStruct(o.shape, o.dtype) for o in outs),
        in_specs=[vmem] * 3,
        out_specs=(hbm,) * 3,
        scratch_shapes=[dma((3,))],
    )(*outs)
    return result, new_state, new_conv.transpose(1, 0, 2)


def solution(mesh):
    in_specs = (
        P(("ep", "tp"), None),
        P("ep", "tp"),
        P("ep", None, "tp"),
        P("ep", None),
        P(("ep", "tp"), None),
        P(),
        P(None, "tp"),
        P(None, "tp"),
        P(),
        P(),
        P(),
        P(),
        P(),
        P("tp", None),
        P(),
        P("ep", None, "tp"),
        P("ep", None, "tp"),
        P("ep", "tp", None),
    )
    out_specs = (P(("ep", "tp"), None), P("ep", "tp"), P("ep", None, "tp"))
    return jax.shard_map(
        per_device, mesh=mesh, in_specs=in_specs, out_specs=out_specs, check_vma=False
    )
```
